512 devices in a mesh: grp: 2 (over y), sp: 16 (over z), tp: 16 (over x, core).
Axes of the slice: x: 8, y: 2, z: 16, core: 2. Of those that a mesh axis runs over, the one named last changes fastest.
The devices are a block of a 8x8x16 slice.
Arguments:
- latent: bfloat16 [16384, 2048], P(('grp', 'sp', 'tp')), parts along dimension 0, may hold values from -3 to 3
- context: bfloat16 [1024, 2048], P(('grp', 'sp')), parts along dimension 0, may hold values from -6 to 6
- condition: float32 [4096], P(('grp', 'sp')), parts along dimension 0, may hold values from -6 to 6
- context_condition: float32 [2048], P('sp'), may hold values from -6 to 6
- mod_weight: bfloat16 [2048, 6144], P('sp', 'tp'), may hold values from -0.1875 to 0.1875
- mod_bias: float32 [6144], replicated, may hold values from -1.5 to 1.5
- query_weight: bfloat16 [2048, 1024], P('sp'), may hold values from -0.125 to 0.125
- key_weight: bfloat16 [2048, 1024], P('sp'), may hold values from -0.125 to 0.125
- value_weight: bfloat16 [2048, 2048], P(None, 'tp'), may hold values from -3 to 3
- out_gate_weight: bfloat16 [2048, 2048], P(None, 'tp'), may hold values from -0.125 to 0.125
- decay_in_weight: bfloat16 [2048, 32], replicated, may hold values from -0.125 to 0.125
- decay_weight: bfloat16 [2, 16, 1024], replicated, may hold values from -1.5 to 1.5
- decay_bias: float32 [2, 1024], replicated, may hold values from 0.5 to 11
- extra_decay: float32 [2, 4, 8192], P(None, None, 'sp'), may hold values from -2.1 to 0
- norm_gain: float32 [512], replicated, may hold values from 0.1 to 1.9
- out_weight: bfloat16 [2048, 2048], P('tp'), may hold values from -0.25 to 0.25
- final_gain: float32 [2048], replicated, may hold values from 0.1 to 1.9
- final_bias: float32 [2048], replicated, may hold values from -1.5 to 1.5
Outputs:
- output: bfloat16 [16384, 2048], P(('grp', 'sp', 'tp')), parts along dimension 0
The draws below stay inside these ranges and needn't reach their ends.
There are 2 independent parts, one for each index of `grp`. The reference program is written for one: setup_inputs(seed, part) draws one part's arguments, and reference() takes and returns one part's arrays. A program takes and returns all parts, laid end to end along the dimension named above; an argument that names none is the same for every part. Nothing has to cross between parts.
All inputs are finite; a program needn't handle non-finite values.
Results may differ from the reference program's by a relative error of at most 0.012.
The reference program's roundings to bfloat16 on the way count: a program that leaves them out, or rounds other values in their place, can miss the bound.
Values may be sent and summed in bfloat16 or wider, within the bound.
A program may use at most 64 MiB of HBM per device.

```python
import math
import jax
import jax.numpy as jnp
from jax import lax

D = 2048
ATTENTION_HEADS = 4
DK = 256
DV = 512
RANK = 16
BLOCK = 64
GRID_W = 64
CTX = 512
TOK_SP = 512
LATENT_TOKENS = 8192
QK = 1024
VD = 2048


def draw_value_weight(key, part):
    noise = jax.random.truncated_normal(key, -4.0, 4.0, (D, ATTENTION_HEADS * DV), jnp.float32)
    column = (jnp.arange(ATTENTION_HEADS * DV) % DV).astype(jnp.float32)
    rising = 4.0 ** (column / DV)
    return (noise * rising * (0.6 / math.sqrt(D))).astype(jnp.bfloat16)


def draw_decay_bias(key, part):
    choose_key, slow_key, fast_key = jax.random.split(key, 3)
    fast_share = 0.5
    picked = jax.random.uniform(choose_key, (2, ATTENTION_HEADS * DK), jnp.float32) < fast_share
    slow_values = jax.random.uniform(slow_key, (2, ATTENTION_HEADS * DK), jnp.float32, 9.0, 11.0)
    fast_values = jax.random.uniform(fast_key, (2, ATTENTION_HEADS * DK), jnp.float32, 0.5, 2.0)
    return jnp.where(picked, fast_values, slow_values)


def draw_extra_decay(key, part):
    rate_key, location_key, keep_key = jax.random.split(key, 3)
    blocks = LATENT_TOKENS // TOK_SP
    rate_values = jnp.exp(jax.random.uniform(rate_key, (2, ATTENTION_HEADS, blocks), jnp.float32, math.log(0.15), math.log(0.9)))
    stable_part = -jnp.repeat(rate_values, TOK_SP, axis=2) / LATENT_TOKENS
    spike_locations = jax.random.randint(location_key, (2, ATTENTION_HEADS, 3), 0, LATENT_TOKENS)
    retain_fraction = jax.random.uniform(keep_key, (2, ATTENTION_HEADS, 3), jnp.float32, 0.5, 0.8)
    token_places = jnp.arange(LATENT_TOKENS)
    match_lookup = token_places[None, None, None, :] == spike_locations[:, :, :, None]
    spike_events = jnp.sum(jnp.where(match_lookup, jnp.log(retain_fraction)[:, :, :, None], 0.0), axis=2)
    return stable_part + spike_events


def steps_of(key, extent, cuts, least, high):
    def one(position, shards_of):
        heights = jax.random.uniform(jax.random.fold_in(jax.random.fold_in(key, 6), position), (shards_of,), jnp.float32, least / len(cuts), high / len(cuts))
        return jnp.repeat(jnp.exp(heights), extent[position] // shards_of).reshape((-1,) + (1,) * (len(extent) - position - 1))

    loudness = one(*cuts[0])
    for cut in cuts[1:]:
        loudness = loudness * one(*cut)
    return loudness


def gaussian(key, dims, scale, limit, pieces=(), kind=jnp.bfloat16):
    values = scale * jax.random.normal(key, dims, jnp.float32)
    if pieces:
        values = values * steps_of(key, dims, pieces, -0.22, 0.18)
    return jnp.clip(values, -limit, limit).astype(kind)


def setup_inputs(seed: int = 0, part: int = 0) -> dict:
    seeds = jax.random.split(jax.random.key(seed), 19)
    own_keys = jax.random.split(jax.random.fold_in(seeds[18], part), 19)
    return {
        "latent": gaussian(own_keys[0], (LATENT_TOKENS, D), 0.5, 3.0, ((0, 256),)),
        "context": gaussian(own_keys[1], (CTX, D), 1.0, 6.0, ((0, 16),)),
        "condition": gaussian(own_keys[2], (D,), 1.0, 6.0, ((0, 16),), jnp.float32),
        "context_condition": gaussian(seeds[3], (D,), 1.0, 6.0, ((0, 16),), jnp.float32),
        "mod_weight": gaussian(seeds[4], (D, 3 * D), (D // 2) ** -0.5, 0.1875, ((0, 16), (1, 16))),
        "mod_bias": gaussian(seeds[5], (3 * D,), 0.3, 1.5, (), jnp.float32),
        "query_weight": gaussian(seeds[6], (D, QK), D ** -0.5, 0.125, ((0, 16),)),
        "key_weight": gaussian(seeds[7], (D, QK), D ** -0.5, 0.125, ((0, 16),)),
        "value_weight": draw_value_weight(jax.random.fold_in(seeds[18], 71), part),
        "out_gate_weight": gaussian(seeds[9], (D, VD), D ** -0.5, 0.125, ((1, 16),)),
        "decay_in_weight": gaussian(seeds[10], (D, 2 * RANK), D ** -0.5, 0.125),
        "decay_weight": gaussian(seeds[11], (2, RANK, QK), RANK ** -0.5, 1.5),
        "decay_bias": draw_decay_bias(jax.random.fold_in(seeds[18], 71), part),
        "extra_decay": draw_extra_decay(jax.random.fold_in(seeds[18], 71), part),
        "norm_gain": jnp.clip(1.0 + 0.18 * jax.random.normal(seeds[14], (DV,), jnp.float32), 0.1, 1.9),
        "out_weight": gaussian(seeds[15], (VD, D), (VD // 4) ** -0.5, 0.25, ((0, 16),)),
        "final_gain": jnp.clip(1.0 + 0.18 * jax.random.normal(seeds[16], (D,), jnp.float32), 0.1, 1.9),
        "final_bias": gaussian(seeds[17], (D,), 0.3, 1.5, (), jnp.float32),
    }


norm_eps = 1e-05
gate_scale = 16.0
rope_base = 10000.0
residual_scale = 2.0 ** 0.5
highest = lax.Precision.HIGHEST

def rotate_half(values, angle):
    half_width = values.shape[-1] // 2
    first_half = values[..., :half_width]
    second_half = values[..., half_width:]
    cosine = jnp.cos(angle)
    sine_part = jnp.sin(angle)
    return jnp.concatenate([first_half * cosine - second_half * sine_part, first_half * sine_part + second_half * cosine], axis=-1)

def rotary(values, token_places):
    quarter = values.shape[-1] // 4
    frequency = rope_base ** (-jnp.arange(quarter, dtype=jnp.float32) / quarter)
    row_index = (token_places // GRID_W).astype(jnp.float32)
    col_index = (token_places % GRID_W).astype(jnp.float32)
    half_width = 2 * quarter
    by_row = rotate_half(values[..., :half_width], row_index[:, None] * frequency)
    by_col = rotate_half(values[..., half_width:], col_index[:, None] * frequency)
    return jnp.concatenate([by_row, by_col], axis=-1)

def log_decays(low_rank, decay_weight, decay_bias):
    rank_width = decay_weight.shape[1]
    decay_parts = []
    for direction in range(2):
        logits = jnp.dot(low_rank[:, direction * rank_width:(direction + 1) * rank_width], decay_weight[direction], preferred_element_type=jnp.float32) + decay_bias[direction]
        decay_parts.append(jax.nn.log_sigmoid(logits) / gate_scale)
    return decay_parts

def by_head(rows, size):
    return rows.astype(jnp.float32).reshape(rows.shape[0], -1, size).transpose(1, 0, 2)

def flip_rows(values):
    return jnp.flip(values, axis=1)

def end_state(key_heads, value_heads, logdec):
    cumulative = jnp.cumsum(logdec, axis=1)
    weights = jnp.exp(cumulative[:, -1:] - cumulative)
    return jnp.einsum('hnd,hnv->hdv', key_heads * weights, value_heads, precision=highest)

def blocked_scan(queries, key_heads, value_heads, logdec, start):
    heads, length, unused_width = queries.shape
    block_count = length // BLOCK
    lower_mask = jnp.tril(jnp.ones((BLOCK, BLOCK), dtype=bool))

    def blocks(values):
        return jnp.moveaxis(values.reshape(heads, block_count, BLOCK, values.shape[-1]), 1, 0)

    def advance(carry_state, block_data):
        query_block, key_block, value_block, decay_block = block_data
        cumulative = jnp.cumsum(decay_block, axis=1)
        total_decay = cumulative[:, -1:]
        query_decayed = query_block * jnp.exp(cumulative)
        key_inverse = key_block * jnp.exp(-cumulative)
        key_closing = key_block * jnp.exp(total_decay - cumulative)
        scores = jnp.einsum('hcd,hsd->hcs', query_decayed, key_inverse, precision=highest)
        scores = jnp.where(lower_mask[None], scores, 0.0)
        outputs = jnp.einsum('hcs,hsv->hcv', scores, value_block, precision=highest) + jnp.einsum('hcd,hdv->hcv', query_decayed, carry_state, precision=highest)
        carry_state = jnp.exp(total_decay)[:, 0, :, None] * carry_state + jnp.einsum('hcd,hcv->hdv', key_closing, value_block, precision=highest)
        return (carry_state, outputs)
    unused_state, outputs = lax.scan(advance, start, (blocks(queries), blocks(key_heads), blocks(value_heads), blocks(logdec)))
    return jnp.moveaxis(outputs, 0, 1).reshape(heads, length, value_heads.shape[-1])

def reference(latent, context, condition, context_condition, mod_weight, mod_bias, query_weight, key_weight, value_weight, out_gate_weight, decay_in_weight, decay_weight, decay_bias, extra_decay, norm_gain, out_weight, final_gain, final_bias):
    model_width = latent.shape[1]
    activated = jax.nn.silu(jnp.stack([condition, context_condition])).astype(jnp.bfloat16)
    modulation = jnp.dot(activated, mod_weight, preferred_element_type=jnp.float32) + mod_bias
    shifts = modulation[:, :model_width]
    scales = modulation[:, model_width:2 * model_width]
    branch_gate = modulation[0, 2 * model_width:]
    mod_latent = (latent.astype(jnp.float32) * (1.0 + scales[0]) + shifts[0]).astype(jnp.bfloat16)
    mod_context = (context.astype(jnp.float32) * (1.0 + scales[1]) + shifts[1]).astype(jnp.bfloat16)

    def project(rows, weight):
        return jnp.dot(rows, weight, preferred_element_type=jnp.float32).astype(jnp.bfloat16)
    queries = project(mod_latent, query_weight)
    out_gate = project(mod_latent, out_gate_weight)
    key_rows = project(mod_latent, key_weight)
    value_rows = project(mod_latent, value_weight)
    low_rank = project(mod_latent, decay_in_weight)
    context_keys = project(mod_context, key_weight)
    context_values = project(mod_context, value_weight)
    context_low = project(mod_context, decay_in_weight)
    token_places = jnp.arange(LATENT_TOKENS, dtype=jnp.int32)
    query_heads = rotary(by_head(queries, DK) * DK ** (-0.5), token_places)
    key_heads = rotary(by_head(key_rows, DK), token_places)
    value_heads = by_head(value_rows, DV)
    latent_decay = log_decays(low_rank, decay_weight, decay_bias)
    forward_decay = by_head(latent_decay[0], DK) + extra_decay[0][:, :, None]
    backward_decay = by_head(latent_decay[1], DK) + extra_decay[1][:, :, None]
    context_decay = log_decays(context_low, decay_weight, decay_bias)
    ctx_key_heads = by_head(context_keys, DK)
    ctx_value_heads = by_head(context_values, DV)
    start_forward = end_state(ctx_key_heads, ctx_value_heads, by_head(context_decay[0], DK))
    start_backward = end_state(flip_rows(ctx_key_heads), flip_rows(ctx_value_heads), flip_rows(by_head(context_decay[1], DK)))
    out_forward = blocked_scan(query_heads, key_heads, value_heads, forward_decay, start_forward)
    out_backward = flip_rows(blocked_scan(flip_rows(query_heads), flip_rows(key_heads), flip_rows(value_heads), flip_rows(backward_decay), start_backward))
    mixture = out_forward + out_backward
    normed = mixture * lax.rsqrt(lax.optimization_barrier(jnp.mean(mixture * mixture, axis=-1, keepdims=True)) + norm_eps) * norm_gain
    normed = normed.transpose(1, 0, 2).reshape(LATENT_TOKENS, ATTENTION_HEADS * DV)
    gated_rows = (normed * jax.nn.silu(out_gate.astype(jnp.float32))).astype(jnp.bfloat16)
    branch = jnp.dot(gated_rows, out_weight, preferred_element_type=jnp.float32)
    summed = residual_scale * latent.astype(jnp.float32) + branch_gate * branch
    row_mean = lax.optimization_barrier(jnp.mean(summed, axis=1, keepdims=True))
    centered = summed - row_mean
    variance = lax.optimization_barrier(jnp.mean(centered * centered, axis=1, keepdims=True))
    return (centered * lax.rsqrt(variance + norm_eps) * final_gain + final_bias).astype(jnp.bfloat16)
```

```python
import functools

import numpy as np
import jax
import jax.numpy as jnp
from jax import lax
from jax.experimental import pallas as pl
from jax.experimental.pallas import tpu as pltpu
from jax.sharding import PartitionSpec as P

ATTENTION_HEADS = 4
DV = 512
BLOCK = 64
GRID_W = 64

norm_eps = 1e-05
gate_scale = 16.0
rope_base = 10000.0
residual_scale = 2.0**0.5
highest = lax.Precision.HIGHEST
f32 = jnp.float32
bf16 = jnp.bfloat16

NT = (((1,), (1,)), ((), ()))
TN = (((0,), (0,)), ((), ()))


def dot(a, b, dims=None, precision=None):
    if dims is None:
        dims = (((1,), (0,)), ((), ()))
    return lax.dot_general(a, b, dims, precision=precision, preferred_element_type=f32)


def log_sigmoid(v):
    return jnp.minimum(v, 0.0) - jnp.log1p(jnp.exp(-jnp.abs(v)))


def silu(v):
    return v / (1.0 + jnp.exp(-v))


def rotary_tables(rows, half):
    quarter = half // 2
    frequency = (rope_base ** (-np.arange(quarter, dtype=np.float64) / quarter)).astype(np.float32)

    def table(places):
        angle = (np.arange(places, dtype=np.float32)[:, None] * frequency).astype(np.float64)
        cosine = np.cos(angle)
        sine = np.sin(angle)
        return np.stack(
            [np.concatenate([cosine, cosine], 1), np.concatenate([-sine, sine], 1)]
        ).astype(np.float32)

    return table(rows), table(GRID_W)


def kernel(
    nz,
    nt,
    heads,
    lat_in,
    ctx_hbm,
    cond,
    ctx_cond,
    mod_w,
    mod_b,
    qw,
    kw,
    vw,
    gw,
    low_hbm,
    decay_w,
    decay_b,
    extra,
    gain,
    out_w,
    final_g,
    final_b,
    row_hbm,
    col_hbm,
    out,
    L,
    XM,
    W,
    VG,
    WO,
    M,
    mod_part,
    PVG,
    PQK,
    QF,
    QD,
    O,
    U,
    TD,
    PF,
    OFF,
    LM,
    LR,
    CM,
    CR,
    DM,
    DR,
    RO,
    RR,
    SS,
    GT,
    GR,
    ACC,
    PS,
    PR,
    CX,
    LOWT,
    RT,
    CT,
    EC,
    EI,
    EO,
    loc_sem,
    once_s,
    once_r,
    wz_r,
    lx_r,
):
    z = lax.axis_index("sp")
    t = lax.axis_index("tp")
    share = nt // heads
    h = t // share
    p = t % share
    core = t % 2
    x = t // 2
    nx = nt // 2
    partner = t + 1 - 2 * core
    D = lat_in.shape[1]
    TB = lat_in.shape[0]
    tok = TB * nt
    KR = qw.shape[0]
    DK = qw.shape[1] // heads
    HC = DK // 2
    VC = vw.shape[1]
    MC = mod_w.shape[1]
    nb = tok // BLOCK
    dvs = VC // nz
    pending = []
    MP, MG, WZ, WD, LX, LD, WOUT, LMS, CMS, DMS, ROS, SSS, GRS, PRS = range(14)

    def push(src, dst, ssem, rsem, **where):
        pltpu.make_async_remote_copy(
            src_ref=src,
            dst_ref=dst,
            send_sem=ssem,
            recv_sem=rsem,
            device_id=where,
            device_id_type=pl.DeviceIdType.MESH,
        ).start()

    def waiter(view, ssem, rsem):
        return pltpu.make_async_remote_copy(
            src_ref=view,
            dst_ref=view,
            send_sem=ssem,
            recv_sem=rsem,
            device_id={"tp": partner},
            device_id_type=pl.DeviceIdType.MESH,
        )

    def all_in(kind, view):
        waiter(view, once_s.at[kind], once_r.at[kind]).wait_recv()

    def sent(kind, view):
        pending.append(waiter(view, once_s.at[kind], once_r.at[kind]))

    def far_first(n):
        return sorted(range(1, n), key=lambda i: (-min(i, n - i), i))

    def at_z(i):
        return lax.rem(z + i + nz, nz)

    def at_t(i):
        return lax.rem(t + i + nt, nt)

    def at_x(i):
        return lax.rem(x + i + nx, nx)

    def al(v, m):
        return pl.multiple_of(v, m)

    barrier = pltpu.get_barrier_semaphore()
    for i in range(1, nz):
        pl.semaphore_signal(
            barrier, inc=1, device_id={"sp": at_z(i)}, device_id_type=pl.DeviceIdType.MESH
        )
    for i in range(1, nt):
        pl.semaphore_signal(
            barrier, inc=1, device_id={"tp": at_t(i)}, device_id_type=pl.DeviceIdType.MESH
        )

    def w_at(zz, j, cc):
        return W.at[pl.ds(al(zz * KR, KR), KR), pl.ds(al(j * DK + cc * HC, HC), HC)]

    def l_at(xx, j, cc):
        return L.at[pl.ds(al((xx * 2 + cc) * TB, TB), TB), pl.ds(j * (D // 2), D // 2)]

    own_cols = pl.ds(al(h * DK + core * HC, HC), HC)
    local = [
        pltpu.make_async_copy(qw.at[:, own_cols], w_at(z, 0, core), loc_sem.at[0]),
        pltpu.make_async_copy(kw.at[:, own_cols], w_at(z, 1, core), loc_sem.at[1]),
        pltpu.make_async_copy(lat_in, L.at[pl.ds(al(t * TB, TB), TB), :], loc_sem.at[2]),
        pltpu.make_async_copy(vw, VG.at[:, pl.ds(0, VC)], loc_sem.at[3]),
        pltpu.make_async_copy(gw, VG.at[:, pl.ds(VC, VC)], loc_sem.at[4]),
        pltpu.make_async_copy(out_w, WO.at[pl.ds(al(p * VC, VC), VC), :], loc_sem.at[5]),
        pltpu.make_async_copy(ctx_hbm, CX, loc_sem.at[6]),
        pltpu.make_async_copy(low_hbm, LOWT, loc_sem.at[7]),
        pltpu.make_async_copy(row_hbm, RT, loc_sem.at[8]),
        pltpu.make_async_copy(col_hbm, CT, loc_sem.at[9]),
    ]
    for copy in local:
        copy.start()

    both = jnp.concatenate([cond[...], ctx_cond[...], jnp.zeros((6, cond.shape[1]), f32)], axis=0)
    part = dot(silu(both).astype(bf16), mod_w[...])
    mod_part[z] = part[0:2]

    for copy in local[:3]:
        copy.wait()
    pl.semaphore_wait(barrier, nz - 1 + nt - 1)

    for i in far_first(nz):
        push(mod_part.at[z], mod_part.at[z], once_s.at[MP], once_r.at[MP], sp=at_z(i))
    sent(MP, mod_part.at[pl.ds(0, nz - 1)])

    def ring(n, at, region, far, sem_r, kind, share_kind):
        long, short = n // 2, (n - 1) // 2

        def last(direction, j):
            return long if direction == j else short

        def index(direction, k, j):
            return (k - 1) * 4 + direction * 2 + j

        def send(direction, k, j):
            src = region(at(-k if direction == 0 else k), j, core)
            push(
                src,
                src,
                once_s.at[kind],
                sem_r.at[index(direction, k + 1, j)],
                **far(1 if direction == 0 else -1),
            )

        def give(xx, j):
            src = region(xx, j, core)
            push(src, src, once_s.at[share_kind], once_r.at[share_kind], tp=partner)

        def step(k):
            for j in range(2):
                for direction in range(2):
                    if 0 < k <= last(direction, j):
                        xx = at(-k if direction == 0 else k)
                        sem = sem_r.at[index(direction, k, j)]
                        waiter(region(xx, j, core), once_s.at[kind], sem).wait_recv()
                    if k < last(direction, j):
                        send(direction, k, j)
                for direction in range(2):
                    if 0 < k <= last(direction, j):
                        give(at(-k if direction == 0 else k), j)

        def start():
            step(0)

        def share_own():
            for j in range(2):
                give(at(0), j)

        return start, share_own, step, long

    l_start, l_own, l_step, l_last = ring(
        nx, at_x, l_at, lambda i: {"tp": at_x(i) * 2 + core}, lx_r, LX, LD
    )
    w_start, w_own, w_step, w_last = ring(nz, at_z, w_at, lambda i: {"sp": at_z(i)}, wz_r, WZ, WD)
    w_start()
    l_start()
    w_own()
    l_own()
    sent(WZ, W.at[pl.ds(0, (nz - 1) * KR), pl.ds(0, DK)])
    sent(WD, W.at[:, pl.ds(0, DK)])
    sent(LX, L.at[pl.ds(0, (nx - 1) * TB), :])
    sent(LD, L.at[pl.ds(0, nx * TB), :])

    def modulation_sums():
        all_in(MP, mod_part.at[pl.ds(0, nz - 1)])
        sums = mod_part[0]
        for i in range(1, nz):
            sums = sums + mod_part[i]
        cols = pl.ds(al(t * MC, 128), MC)
        M[:, cols] = sums
        for i in far_first(nt):
            push(M.at[:, cols], M.at[:, cols], once_s.at[MG], once_r.at[MG], tp=at_t(i))
        sent(MG, M.at[:, pl.ds(0, (nt - 1) * MC)])

    w_done = 0
    for k in range(1, l_last + 1):
        if k <= w_last:
            w_step(k)
            w_done = k
        l_step(k)
        if k == min(3, l_last):
            modulation_sums()
    local[5].wait()
    own_rows = WO.at[pl.ds(al(p * VC, VC), VC), :]
    for i in range(1, share):
        push(
            own_rows,
            own_rows,
            once_s.at[WOUT],
            once_r.at[WOUT],
            tp=h * share + lax.rem(p + i, share),
        )
    sent(WOUT, WO.at[pl.ds(0, (share - 1) * VC), :])
    all_in(LD, L.at[pl.ds(0, nx * TB), :])
    all_in(MG, M.at[:, pl.ds(0, (nt - 1) * MC)])
    for copy in local[3:5] + local[6:]:
        copy.wait()

    mod = M[...] + mod_b[...]
    shift, scale = mod[:, :D], 1.0 + mod[:, D : 2 * D]
    bias = decay_b[:, pl.ds(al(h * DK, DK), DK)]
    rank = decay_w.shape[1]
    zero = jnp.zeros((rank, DK), bf16)
    head_cols = pl.ds(al(h * DK, DK), DK)
    maps = [
        jnp.concatenate([decay_w[0, :, head_cols], zero], axis=0),
        jnp.concatenate([zero, decay_w[1, :, head_cols]], axis=0),
    ]

    def triangles(size):
        row = lax.broadcasted_iota(jnp.int32, (size, size), 0)
        col = lax.broadcasted_iota(jnp.int32, (size, size), 1)
        return row >= col, row <= col

    low_b, up_b = triangles(BLOCK)
    added = [extra[d, pl.ds(h, 1), :] for d in range(2)]

    def decays(low, d):
        return log_sigmoid(dot(low, maps[d]) + bias[d : d + 1]) * (1.0 / gate_scale)

    tiles = max(1, tok // 128)
    TR = tok // tiles

    def project_tile(i):
        rows = pl.ds(i * TR, TR)
        rounded = (L[rows, :].astype(f32) * scale[0:1] + shift[0:1]).astype(bf16)
        XM[rows, :] = rounded
        PVG[rows, :] = dot(rounded, VG[...]).astype(bf16)
        low = dot(rounded, LOWT[...], NT).astype(bf16)
        for d, mask in ((0, low_b), (1, up_b)):
            steps = decays(low, d)
            for b in range(i * TR // BLOCK, (i + 1) * TR // BLOCK):
                at = b * BLOCK - i * TR
                ex = added[d][:, b * BLOCK : (b + 1) * BLOCK]
                cum = dot(mask.astype(f32), steps[at : at + BLOCK], precision=highest) + jnp.sum(
                    jnp.where(mask, ex, 0.0), axis=1, keepdims=True
                )
                total = cum[BLOCK - 1 : BLOCK] if d == 0 else cum[0:1]
                block_rows = slice(b * BLOCK, (b + 1) * BLOCK)
                EC[d, block_rows, :] = jnp.exp(cum)
                EI[d, block_rows, :] = jnp.exp(-cum)
                EO[d, block_rows, :] = jnp.exp(total - cum)
                TD[d, b] = total

    tile = 0
    for k in range(w_done + 1, w_last + 1):
        if tile < tiles:
            project_tile(tile)
            tile += 1
        w_step(k)
    while tile < tiles:
        project_tile(tile)
        tile += 1

    ctx_rows = (CX[...].astype(f32) * scale[1:2] + shift[1:2]).astype(bf16)
    ctx_values = dot(ctx_rows, VG[:, 0:VC]).astype(bf16)
    ctx_low = dot(ctx_rows, LOWT[...], NT).astype(bf16)
    CB = ctx_hbm.shape[0]
    low_c, up_c = triangles(CB)
    cum_f = dot(low_c.astype(f32), decays(ctx_low, 0), precision=highest)
    cum_b = dot(up_c.astype(f32), decays(ctx_low, 1), precision=highest)
    tot_cf, tot_cb = cum_f[CB - 1 : CB], cum_b[0:1]
    sum_f, sum_b = jnp.zeros((1, DK), f32), jnp.zeros((1, DK), f32)
    for b in range(nb):
        OFF[0, b] = sum_f
        OFF[1, nb - 1 - b] = sum_b
        sum_f = sum_f + TD[0, b]
        sum_b = sum_b + TD[1, nb - 1 - b]
    DM[...] = jnp.concatenate([sum_f, sum_b, tot_cf, tot_cb], axis=0)
    for i in far_first(nz):
        push(DM, DR.at[z], once_s.at[DMS], once_r.at[DMS], sp=at_z(i))
    sent(DMS, DR.at[pl.ds(0, nz - 1)])
    DR[z] = DM[...]
    all_in(WD, W.at[:, pl.ds(0, DK)])

    def message(forward, backward):
        return jnp.concatenate(
            [forward.reshape(nz, dvs, DK), backward.reshape(nz, dvs, DK)], axis=1
        ).astype(bf16)

    ctx_keys = dot(ctx_rows, W[:, DK : 2 * DK]).astype(bf16).astype(f32)
    CM[...] = message(
        dot(ctx_values, (ctx_keys * jnp.exp(tot_cf - cum_f)).astype(bf16), TN),
        dot(ctx_values, (ctx_keys * jnp.exp(tot_cb - cum_b)).astype(bf16), TN),
    )
    for i in far_first(nz):
        push(CM.at[at_z(i)], CR.at[z], once_s.at[CMS], once_r.at[CMS], sp=at_z(i))
    sent(CMS, CM.at[pl.ds(0, nz - 1)])
    CR[z] = CM[z]

    QT = min(tok, 256)

    def project_qk(i, carry):
        rows = pl.ds(al(i * QT, QT), QT)
        PQK[rows, :] = dot(XM[rows, :], W[...]).astype(bf16)
        return carry

    lax.fori_loop(0, tok // QT, project_qk, 0)

    half = DK // 2
    for b in range(nb):
        rows = slice(b * BLOCK, (b + 1) * BLOCK)
        place = pl.ds(z * nb + b, 1)
        row_cos, row_sin = RT[0, place, :], RT[1, place, :]

        def rotated(values):
            first, second = values[:, :half], values[:, half:]
            return jnp.concatenate(
                [
                    first * row_cos + pltpu.roll(first, half // 2, 1) * row_sin,
                    second * CT[0] + pltpu.roll(second, half // 2, 1) * CT[1],
                ],
                axis=1,
            )

        q = rotated(PQK[rows, :DK].astype(f32)) * DK ** (-0.5)
        k = rotated(PQK[rows, DK:].astype(f32))
        v = PVG[rows, 0:VC]
        scores = None
        for d, mask in ((0, low_b), (1, up_b)):
            q_in = (q * EC[d, rows, :]).astype(bf16)
            k_in = (k * EI[d, rows, :]).astype(bf16)
            k_out = (k * EO[d, rows, :]).astype(bf16)
            QF[rows, d * DK : (d + 1) * DK] = q_in
            U[d, b] = dot(v, k_out, TN)
            one = jnp.where(mask, dot(q_in, k_in, NT), 0.0)
            scores = one if scores is None else scores + one
        O[rows, :] = dot(scores.astype(bf16), v)

    fwd, bwd = jnp.zeros((VC, DK), f32), jnp.zeros((VC, DK), f32)
    for b in range(nb):
        e = nb - 1 - b
        PF[0, b] = fwd.astype(bf16)
        PF[1, e] = bwd.astype(bf16)
        fwd = jnp.exp(TD[0, b]) * fwd + U[0, b]
        bwd = jnp.exp(TD[1, e]) * bwd + U[1, e]
    LM[...] = message(fwd, bwd)
    for i in far_first(nz):
        push(LM.at[at_z(i)], LR.at[z], once_s.at[LMS], once_r.at[LMS], sp=at_z(i))
    sent(LMS, LM.at[pl.ds(0, nz - 1)])
    LR[z] = LM[z]

    def inner(b, carry):
        rows = pl.ds(al(b * BLOCK, BLOCK), BLOCK)
        total = O[rows, :]
        for d in range(2):
            cols = slice(d * DK, (d + 1) * DK)
            q_in = QF[rows, cols]
            total = total + dot(q_in, PF[d, b], NT)
            QD[rows, cols] = (q_in.astype(f32) * jnp.exp(OFF[d, b])).astype(bf16)
        O[rows, :] = total
        return carry

    lax.fori_loop(0, nb, inner, 0)

    all_in(CMS, CR.at[pl.ds(0, nz - 1)])
    all_in(DMS, DR.at[pl.ds(0, nz - 1)])
    all_in(LMS, LR.at[pl.ds(0, nz - 1)])

    def context_chain(s, carry):
        fwd, bwd = carry
        e = nz - 1 - s
        fwd = jnp.exp(DR[s, 2:3]) * fwd + CR[s].astype(f32)[:dvs]
        bwd = jnp.exp(DR[e, 3:4]) * bwd + CR[e].astype(f32)[dvs:]
        return fwd, bwd

    slice0 = jnp.zeros((dvs, DK), f32)
    fwd, bwd = lax.fori_loop(0, nz, context_chain, (slice0, slice0))
    fwd_in, bwd_in = [], [None] * nz
    for s in range(nz):
        e = nz - 1 - s
        fwd_in.append(fwd)
        bwd_in[e] = bwd
        fwd = jnp.exp(DR[s, 0:1]) * fwd + LR[s].astype(f32)[:dvs]
        bwd = jnp.exp(DR[e, 1:2]) * bwd + LR[e].astype(f32)[dvs:]
    for s in range(nz):
        RO[s] = jnp.concatenate([fwd_in[s], bwd_in[s]], axis=0).astype(bf16)
    for i in far_first(nz):
        push(RO.at[at_z(i)], RR.at[z], once_s.at[ROS], once_r.at[ROS], sp=at_z(i))
    sent(ROS, RO.at[pl.ds(0, nz - 1)])
    RR[z] = RO[z]
    gate_rows = silu(PVG[:, VC:].astype(f32)) * gain[:, pl.ds(al(p * VC, VC), VC)]
    all_in(ROS, RR.at[pl.ds(0, nz - 1)])
    back = RR[...].astype(f32)
    start = jnp.concatenate(
        [back[:, :dvs].reshape(VC, DK), back[:, dvs:].reshape(VC, DK)], axis=1
    ).astype(bf16)
    mixture = O[...] + dot(QD[...], start, NT)

    SS[p] = dot(jnp.ones((8, VC), f32), mixture * mixture, NT, precision=highest)
    for i in range(1, share):
        push(
            SS.at[p],
            SS.at[p],
            once_s.at[SSS],
            once_r.at[SSS],
            tp=h * share + lax.rem(p + i, share),
        )
    sent(SSS, SS.at[pl.ds(0, share - 1)])
    unscaled = mixture * gate_rows
    all_in(SSS, SS.at[pl.ds(0, share - 1)])
    squares = SS[0]
    for i in range(1, share):
        squares = squares + SS[i]
    inverse = lax.rsqrt(squares / (share * VC) + norm_eps)
    gated = (unscaled * inverse.T[:, 0:1]).astype(bf16)
    GT[...] = gated.reshape(heads, share, TB, VC)
    for i in range(1, share):
        q = lax.rem(p + i, share)
        push(
            GT.at[:, q],
            GR.at[:, :, pl.ds(al(p * VC, VC), VC)],
            once_s.at[GRS],
            once_r.at[GRS],
            tp=h * share + q,
        )
    sent(GRS, GT.at[:, pl.ds(0, share - 1)])
    GR[:, :, pl.ds(al(p * VC, VC), VC)] = GT[:, p]
    all_in(WOUT, WO.at[pl.ds(0, (share - 1) * VC), :])
    all_in(GRS, GT.at[:, pl.ds(0, share - 1)])

    left = GR[...].reshape(heads * TB, share * VC)
    NC = D // 4
    for n in range(4):
        cols = slice(n * NC, (n + 1) * NC)
        partial = dot(left, WO[:, cols]).reshape(heads, TB, NC)
        ACC[:, :, cols] = partial
        PS[:, :, cols] = partial.astype(bf16)
    for i in range(1, heads):
        g = lax.rem(h + i, heads)
        push(PS.at[g], PR.at[h], once_s.at[PRS], once_r.at[PRS], tp=g * share + p)
    if heads > 1:
        sent(PRS, PS.at[pl.ds(0, heads - 1)])
        all_in(PRS, PR.at[pl.ds(0, heads - 1)])
    branch = ACC[h]
    for i in range(1, heads):
        g = lax.rem(h - i + heads, heads)
        branch = branch + PR[g].astype(f32)
    own = L[pl.ds(al(t * TB, TB), TB), :].astype(f32)
    gates = M[0:1, 2 * D :] + mod_b[:, 2 * D :]
    summed = residual_scale * own + gates * branch
    centered = summed - jnp.mean(summed, axis=1, keepdims=True)
    variance = jnp.mean(centered * centered, axis=1, keepdims=True)
    out[...] = (
        centered * lax.rsqrt(variance + norm_eps) * final_g[...] + final_b[...]
    ).astype(out.dtype)
    for copy in pending:
        copy.wait_send()


def body(
    nz,
    nt,
    latent,
    context,
    condition,
    context_condition,
    mod_weight,
    mod_bias,
    query_weight,
    key_weight,
    value_weight,
    out_gate_weight,
    decay_in_weight,
    decay_weight,
    decay_bias,
    extra_decay,
    norm_gain,
    out_weight,
    final_gain,
    final_bias,
):
    heads = ATTENTION_HEADS
    share = nt // heads
    D = latent.shape[1]
    TB = latent.shape[0]
    tok = TB * nt
    DK = query_weight.shape[1] // heads
    VC = value_weight.shape[1]
    MC = mod_weight.shape[1]
    nb = tok // BLOCK
    row_tab, col_tab = rotary_tables(nz * nb, DK // 2)
    dvs = VC // nz
    vmem = pl.BlockSpec(memory_space=pltpu.VMEM)
    hbm = pl.BlockSpec(memory_space=pl.ANY)
    dma = pltpu.SemaphoreType.DMA
    scratch = [
        pltpu.VMEM((tok, D), bf16),
        pltpu.VMEM((tok, D), bf16),
        pltpu.VMEM((D, 2 * DK), bf16),
        pltpu.VMEM((D, 2 * VC), bf16),
        pltpu.VMEM((share * VC, D), bf16),
        pltpu.VMEM((2, 3 * D), f32),
        pltpu.VMEM((nz, 2, MC), f32),
        pltpu.VMEM((tok, 2 * VC), bf16),
        pltpu.VMEM((tok, 2 * DK), bf16),
        pltpu.VMEM((tok, 2 * DK), bf16),
        pltpu.VMEM((tok, 2 * DK), bf16),
        pltpu.VMEM((tok, VC), f32),
        pltpu.VMEM((2, nb, VC, DK), f32),
        pltpu.VMEM((2, nb, 1, DK), f32),
        pltpu.VMEM((2, nb, VC, DK), bf16),
        pltpu.VMEM((2, nb, 1, DK), f32),
        pltpu.VMEM((nz, 2 * dvs, DK), bf16),
        pltpu.VMEM((nz, 2 * dvs, DK), bf16),
        pltpu.VMEM((nz, 2 * dvs, DK), bf16),
        pltpu.VMEM((nz, 2 * dvs, DK), bf16),
        pltpu.VMEM((4, DK), f32),
        pltpu.VMEM((nz, 4, DK), f32),
        pltpu.VMEM((nz, 2 * dvs, DK), bf16),
        pltpu.VMEM((nz, 2 * dvs, DK), bf16),
        pltpu.VMEM((share, 8, tok), f32),
        pltpu.VMEM((heads, share, TB, VC), bf16),
        pltpu.VMEM((heads, TB, share * VC), bf16),
        pltpu.VMEM((heads, TB, D), f32),
        pltpu.VMEM((heads, TB, D), bf16),
        pltpu.VMEM((heads, TB, D), bf16),
        pltpu.VMEM(context.shape, bf16),
        pltpu.VMEM((decay_in_weight.shape[1], D), bf16),
        pltpu.VMEM(row_tab.shape, f32),
        pltpu.VMEM(col_tab.shape, f32),
        pltpu.VMEM((2, tok, DK), f32),
        pltpu.VMEM((2, tok, DK), f32),
        pltpu.VMEM((2, tok, DK), f32),
        dma((10,)),
        dma((14,)),
        dma((14,)),
        dma((4 * (nz // 2),)),
        dma((4 * (nt // 4),)),
    ]
    in_specs = [vmem] * 20
    for index in (0, 1, 6, 7, 8, 9, 10, 15, 18, 19):
        in_specs[index] = hbm
    return pl.pallas_call(
        functools.partial(kernel, nz, nt, heads),
        out_shape=jax.ShapeDtypeStruct((TB, D), bf16),
        in_specs=in_specs,
        out_specs=vmem,
        scratch_shapes=scratch,
        compiler_params=pltpu.CompilerParams(
            collective_id=0, has_side_effects=True, vmem_limit_bytes=58 * 1024 * 1024
        ),
        name="layer",
    )(
        latent,
        context,
        condition.reshape(1, -1),
        context_condition.reshape(1, -1),
        mod_weight,
        mod_bias.reshape(1, -1),
        query_weight,
        key_weight,
        value_weight,
        out_gate_weight,
        decay_in_weight.T,
        decay_weight,
        decay_bias,
        extra_decay,
        norm_gain.reshape(1, -1),
        out_weight,
        final_gain.reshape(1, -1),
        final_bias.reshape(1, -1),
        jnp.asarray(row_tab),
        jnp.asarray(col_tab),
    )


def solution(mesh):
    placed = (
        P(("grp", "sp", "tp"), None),
        P(("grp", "sp"), None),
        P(("grp", "sp")),
        P("sp"),
        P("sp", "tp"),
        P(),
        P("sp", None),
        P("sp", None),
        P(None, "tp"),
        P(None, "tp"),
        P(),
        P(),
        P(),
        P(None, None, "sp"),
        P(),
        P("tp", None),
        P(),
        P(),
    )
    return jax.shard_map(
        functools.partial(body, mesh.shape["sp"], mesh.shape["tp"]),
        mesh=mesh,
        in_specs=placed,
        out_specs=P(("grp", "sp", "tp"), None),
        check_vma=False,
    )
```

```python
import functools

import numpy as np
import jax
import jax.numpy as jnp
from jax import lax
from jax.experimental import pallas as pl
from jax.experimental.pallas import tpu as pltpu
from jax.sharding import PartitionSpec as P

ATTENTION_HEADS = 4
DV = 512
BLOCK = 64
GRID_W = 64

norm_eps = 1e-05
gate_scale = 16.0
rope_base = 10000.0
residual_scale = 2.0**0.5
highest = lax.Precision.HIGHEST
f32 = jnp.float32
bf16 = jnp.bfloat16

NT = (((1,), (1,)), ((), ()))
TN = (((0,), (0,)), ((), ()))


def dot(a, b, dims=None, precision=None):
    if dims is None:
        dims = (((1,), (0,)), ((), ()))
    return lax.dot_general(a, b, dims, precision=precision, preferred_element_type=f32)


def log_sigmoid(v):
    return jnp.minimum(v, 0.0) - jnp.log1p(jnp.exp(-jnp.abs(v)))


def silu(v):
    return v / (1.0 + jnp.exp(-v))


def rotary_tables(rows, half):
    quarter = half // 2
    frequency = (rope_base ** (-np.arange(quarter, dtype=np.float64) / quarter)).astype(np.float32)

    def table(places):
        angle = (np.arange(places, dtype=np.float32)[:, None] * frequency).astype(np.float64)
        cosine = np.cos(angle)
        sine = np.sin(angle)
        return np.stack(
            [np.concatenate([cosine, cosine], 1), np.concatenate([-sine, sine], 1)]
        ).astype(np.float32)

    return table(rows), table(GRID_W)


def kernel(
    nz,
    nt,
    heads,
    lat_in,
    ctx_hbm,
    cond_hbm,
    ctx_cond_hbm,
    mod_w_hbm,
    mod_b_hbm,
    qw,
    kw,
    vw,
    gw,
    low_hbm,
    decay_w_hbm,
    decay_b_hbm,
    extra_hbm,
    gain_hbm,
    out_w,
    final_g_hbm,
    final_b_hbm,
    row_hbm,
    col_hbm,
    out,
    L,
    XM,
    W,
    VG,
    WO,
    M,
    mod_part,
    PVG,
    PQK,
    QF,
    QD,
    O,
    U,
    TD,
    PF,
    OFF,
    LM,
    LR,
    CM,
    CR,
    DM,
    DR,
    RO,
    RR,
    SS,
    GT,
    GR,
    ACC,
    PS,
    PR,
    IV,
    cond,
    ctx_cond,
    mod_w,
    mod_b,
    decay_w,
    decay_b,
    extra,
    gain,
    final_g,
    final_b,
    CX,
    LOWT,
    RT,
    CT,
    EC,
    EI,
    EO,
    loc_sem,
    once_s,
    once_r,
    wz_r,
    lx_r,
):
    z = lax.axis_index("sp")
    t = lax.axis_index("tp")
    share = nt // heads
    h = t // share
    p = t % share
    core = t % 2
    x = t // 2
    nx = nt // 2
    partner = t + 1 - 2 * core
    D = lat_in.shape[1]
    TB = lat_in.shape[0]
    tok = TB * nt
    KR = qw.shape[0]
    DK = qw.shape[1] // heads
    HC = DK // 2
    VC = vw.shape[1]
    MC = mod_w_hbm.shape[1]
    nb = tok // BLOCK
    dvs = VC // nz
    pending = []
    MP, MG, WZ, WD, LX, LD, WOUT, LMS, CMS, DMS, ROS, SSS, GRS, PRS = range(14)

    def push(src, dst, ssem, rsem, **where):
        pltpu.make_async_remote_copy(
            src_ref=src,
            dst_ref=dst,
            send_sem=ssem,
            recv_sem=rsem,
            device_id=where,
            device_id_type=pl.DeviceIdType.MESH,
        ).start()

    def waiter(view, ssem, rsem):
        return pltpu.make_async_remote_copy(
            src_ref=view,
            dst_ref=view,
            send_sem=ssem,
            recv_sem=rsem,
            device_id={"tp": partner},
            device_id_type=pl.DeviceIdType.MESH,
        )

    def all_in(kind, view):
        waiter(view, once_s.at[kind], once_r.at[kind]).wait_recv()

    def sent(kind, view):
        pending.append(waiter(view, once_s.at[kind], once_r.at[kind]))

    def far_first(n):
        return sorted(range(1, n), key=lambda i: (-min(i, n - i), i))

    def at_z(i):
        return lax.rem(z + i + nz, nz)

    def at_t(i):
        return lax.rem(t + i + nt, nt)

    def at_x(i):
        return lax.rem(x + i + nx, nx)

    def al(v, m):
        return pl.multiple_of(v, m)

    def w_at(zz, j):
        return W.at[pl.ds(al(zz * KR, KR), KR), pl.ds(j * DK, DK)]

    def l_at(xx, j):
        return L.at[pl.ds(al((xx * 2 + j) * TB, TB), TB), :]

    head_cols = pl.ds(al(h * DK, DK), DK)
    loads = [
        (cond_hbm, cond),
        (ctx_cond_hbm, ctx_cond),
        (mod_w_hbm, mod_w),
        (lat_in, L.at[pl.ds(al(t * TB, TB), TB), :]),
        (qw.at[:, head_cols], w_at(z, 0)),
        (kw.at[:, head_cols], w_at(z, 1)),
        (out_w, WO.at[pl.ds(al(p * VC, VC), VC), :]),
        (vw, VG.at[:, pl.ds(0, VC)]),
        (gw, VG.at[:, pl.ds(VC, VC)]),
        (ctx_hbm, CX),
        (low_hbm, LOWT),
        (mod_b_hbm, mod_b),
        (decay_w_hbm, decay_w),
        (decay_b_hbm, decay_b),
        (extra_hbm, extra),
        (gain_hbm, gain),
        (final_g_hbm, final_g),
        (final_b_hbm, final_b),
        (row_hbm, RT),
        (col_hbm, CT),
    ]
    local = [
        pltpu.make_async_copy(src, dst, loc_sem.at[i]) for i, (src, dst) in enumerate(loads)
    ]
    for copy in local:
        copy.start()

    barrier = pltpu.get_barrier_semaphore()
    for i in far_first(nz):
        pl.semaphore_signal(
            barrier, inc=1, device_id={"sp": at_z(i)}, device_id_type=pl.DeviceIdType.MESH
        )
    for i in far_first(nt):
        pl.semaphore_signal(
            barrier, inc=1, device_id={"tp": at_t(i)}, device_id_type=pl.DeviceIdType.MESH
        )
    for copy in local[:3]:
        copy.wait()

    both = jnp.concatenate([cond[...], ctx_cond[...], jnp.zeros((6, cond.shape[1]), f32)], axis=0)
    part = dot(silu(both).astype(bf16), mod_w[...])
    mod_part[z] = part[0:2]

    for copy in local[3:6]:
        copy.wait()
    pl.semaphore_wait(barrier, nz - 1 + nt - 1)

    for i in far_first(nz):
        push(mod_part.at[z], mod_part.at[z], once_s.at[MP], once_r.at[MP], sp=at_z(i))
    sent(MP, mod_part.at[pl.ds(0, nz - 1)])

    def ring(n, at, region, far, sem_r, kind, share_kind):
        long, short = n // 2, (n - 1) // 2

        def last(direction, j):
            return long if direction == j else short

        def index(direction, k, j):
            return (k - 1) * 4 + direction * 2 + j

        def send(direction, k, j):
            src = region(at(-k if direction == 0 else k), j)
            push(
                src,
                src,
                once_s.at[kind],
                sem_r.at[index(direction, k + 1, j)],
                **far(1 if direction == 0 else -1),
            )

        def give(xx, j):
            src = region(xx, j)
            push(src, src, once_s.at[share_kind], once_r.at[share_kind], tp=partner)

        def step(k):
            for j in range(2):
                for direction in range(2):
                    if 0 < k <= last(direction, j):
                        xx = at(-k if direction == 0 else k)
                        sem = sem_r.at[index(direction, k, j)]
                        waiter(region(xx, j), once_s.at[kind], sem).wait_recv()
                    if k < last(direction, j):
                        send(direction, k, j)
                for direction in range(2):
                    if 0 < k <= last(direction, j):
                        give(at(-k if direction == 0 else k), j)

        return send, give, step, long, last

    l_send, l_give, l_step, l_long, l_last = ring(
        nx, at_x, l_at, lambda i: {"tp": at_x(i) * 2 + core}, lx_r, LX, LD
    )
    w_send, w_give, w_step, w_long, w_last = ring(
        nz, at_z, w_at, lambda i: {"sp": at_z(i)}, wz_r, WZ, WD
    )
    rest = pl.ds(0, (2 * nx - 1) * TB)

    @pl.when(core == 0)
    def _():
        for direction in range(2):
            if l_last(direction, 0):
                l_send(direction, 0, 0)
        l_give(x, 0)
        all_in(LD, L.at[pl.ds(0, TB), :])
        for direction in range(2):
            if l_last(direction, 1):
                l_send(direction, 0, 1)
        for k in range(1, min(2, l_long) + 1):
            l_step(k)

    @pl.when(core == 1)
    def _():
        l_give(x, 1)
        w_step(0)
        for k in range(1, min(3, w_long) + 1):
            w_step(k)

    def modulation_sums():
        all_in(MP, mod_part.at[pl.ds(0, nz - 1)])
        sums = mod_part[0]
        for i in range(1, nz):
            sums = sums + mod_part[i]
        cols = pl.ds(al(t * MC, 128), MC)
        M[:, cols] = sums
        for i in far_first(nt):
            push(M.at[:, cols], M.at[:, cols], once_s.at[MG], once_r.at[MG], tp=at_t(i))
        sent(MG, M.at[:, pl.ds(0, (nt - 1) * MC)])

    modulation_sums()
    w_done = min(5, w_long)

    @pl.when(core == 0)
    def _():
        for k in range(3, l_long + 1):
            l_step(k)

    @pl.when(core == 1)
    def _():
        for k in range(4, w_done + 1):
            w_step(k)

    local[6].wait()
    own_rows = WO.at[pl.ds(al(p * VC, VC), VC), :]
    for i in range(1, share):
        push(
            own_rows,
            own_rows,
            once_s.at[WOUT],
            once_r.at[WOUT],
            tp=h * share + lax.rem(p + i, share),
        )
    sent(WOUT, WO.at[pl.ds(0, (share - 1) * VC), :])
    @pl.when(core == 1)
    def _():
        all_in(LD, L.at[rest, :])

    all_in(MG, M.at[:, pl.ds(0, (nt - 1) * MC)])
    for copy in local[7:]:
        copy.wait()

    mod = M[...] + mod_b[...]
    shift, scale = mod[:, :D], 1.0 + mod[:, D : 2 * D]
    bias = decay_b[:, pl.ds(al(h * DK, DK), DK)]
    rank = decay_w.shape[1]
    zero = jnp.zeros((rank, DK), bf16)
    maps = [
        jnp.concatenate([decay_w[0, :, head_cols], zero], axis=0),
        jnp.concatenate([zero, decay_w[1, :, head_cols]], axis=0),
    ]

    def triangles(size):
        row = lax.broadcasted_iota(jnp.int32, (size, size), 0)
        col = lax.broadcasted_iota(jnp.int32, (size, size), 1)
        return row >= col, row <= col

    low_b, up_b = triangles(BLOCK)
    added = [extra[d, pl.ds(h, 1), :] for d in range(2)]

    def decays(low, d):
        return log_sigmoid(dot(low, maps[d]) + bias[d : d + 1]) * (1.0 / gate_scale)

    tiles = max(1, tok // 128)
    TR = tok // tiles

    def project_tile(i):
        rows = pl.ds(i * TR, TR)
        rounded = (L[rows, :].astype(f32) * scale[0:1] + shift[0:1]).astype(bf16)
        XM[rows, :] = rounded
        PVG[rows, :] = dot(rounded, VG[...]).astype(bf16)
        low = dot(rounded, LOWT[...], NT).astype(bf16)
        for d, mask in ((0, low_b), (1, up_b)):
            steps = decays(low, d)
            for b in range(i * TR // BLOCK, (i + 1) * TR // BLOCK):
                at = b * BLOCK - i * TR
                ex = added[d][:, b * BLOCK : (b + 1) * BLOCK]
                cum = dot(mask.astype(f32), steps[at : at + BLOCK], precision=highest) + jnp.sum(
                    jnp.where(mask, ex, 0.0), axis=1, keepdims=True
                )
                total = cum[BLOCK - 1 : BLOCK] if d == 0 else cum[0:1]
                block_rows = slice(b * BLOCK, (b + 1) * BLOCK)
                EC[d, block_rows, :] = jnp.exp(cum)
                EI[d, block_rows, :] = jnp.exp(-cum)
                EO[d, block_rows, :] = jnp.exp(total - cum)
                TD[d, b] = total

    tile = 0
    for k in range(w_done + 1, w_long + 1):
        if tile < tiles:
            project_tile(tile)
            tile += 1

        @pl.when(core == 1)
        def _():
            w_step(k)

    while tile < tiles:
        project_tile(tile)
        tile += 1

    ctx_rows = (CX[...].astype(f32) * scale[1:2] + shift[1:2]).astype(bf16)
    ctx_values = dot(ctx_rows, VG[:, 0:VC]).astype(bf16)
    ctx_low = dot(ctx_rows, LOWT[...], NT).astype(bf16)
    CB = ctx_hbm.shape[0]
    low_c, up_c = triangles(CB)
    cum_f = dot(low_c.astype(f32), decays(ctx_low, 0), precision=highest)
    cum_b = dot(up_c.astype(f32), decays(ctx_low, 1), precision=highest)
    tot_cf, tot_cb = cum_f[CB - 1 : CB], cum_b[0:1]
    sum_f, sum_b = jnp.zeros((1, DK), f32), jnp.zeros((1, DK), f32)
    for b in range(nb):
        OFF[0, b] = sum_f
        OFF[1, nb - 1 - b] = sum_b
        sum_f = sum_f + TD[0, b]
        sum_b = sum_b + TD[1, nb - 1 - b]
    DM[...] = jnp.concatenate([sum_f, sum_b, tot_cf, tot_cb], axis=0)
    for i in far_first(nz):
        push(DM, DR.at[z], once_s.at[DMS], once_r.at[DMS], sp=at_z(i))
    sent(DMS, DR.at[pl.ds(0, nz - 1)])
    DR[z] = DM[...]
    @pl.when(core == 0)
    def _():
        all_in(WD, W.at[pl.ds(0, (nz - 1) * KR), :])

    def message(forward, backward):
        return jnp.concatenate(
            [forward.reshape(nz, dvs, DK), backward.reshape(nz, dvs, DK)], axis=1
        ).astype(bf16)

    ctx_keys = dot(ctx_rows, W[:, DK : 2 * DK]).astype(bf16).astype(f32)
    CM[...] = message(
        dot(ctx_values, (ctx_keys * jnp.exp(tot_cf - cum_f)).astype(bf16), TN),
        dot(ctx_values, (ctx_keys * jnp.exp(tot_cb - cum_b)).astype(bf16), TN),
    )
    for i in far_first(nz):
        push(CM.at[at_z(i)], CR.at[z], once_s.at[CMS], once_r.at[CMS], sp=at_z(i))
    sent(CMS, CM.at[pl.ds(0, nz - 1)])
    CR[z] = CM[z]

    QT = min(tok, 256)

    def project_qk(i, carry):
        rows = pl.ds(al(i * QT, QT), QT)
        PQK[rows, :] = dot(XM[rows, :], W[...]).astype(bf16)
        return carry

    lax.fori_loop(0, tok // QT, project_qk, 0)

    half = DK // 2
    for b in range(nb):
        rows = slice(b * BLOCK, (b + 1) * BLOCK)
        place = pl.ds(z * nb + b, 1)
        row_cos, row_sin = RT[0, place, :], RT[1, place, :]

        def rotated(values):
            first, second = values[:, :half], values[:, half:]
            return jnp.concatenate(
                [
                    first * row_cos + pltpu.roll(first, half // 2, 1) * row_sin,
                    second * CT[0] + pltpu.roll(second, half // 2, 1) * CT[1],
                ],
                axis=1,
            )

        q = rotated(PQK[rows, :DK].astype(f32)) * DK ** (-0.5)
        k = rotated(PQK[rows, DK:].astype(f32))
        v = PVG[rows, 0:VC]
        scores = None
        for d, mask in ((0, low_b), (1, up_b)):
            q_in = (q * EC[d, rows, :]).astype(bf16)
            k_in = (k * EI[d, rows, :]).astype(bf16)
            k_out = (k * EO[d, rows, :]).astype(bf16)
            QF[rows, d * DK : (d + 1) * DK] = q_in
            U[d, b] = dot(v, k_out, TN)
            one = jnp.where(mask, dot(q_in, k_in, NT), 0.0)
            scores = one if scores is None else scores + one
        O[rows, :] = dot(scores.astype(bf16), v)

    fwd, bwd = jnp.zeros((VC, DK), f32), jnp.zeros((VC, DK), f32)
    for b in range(nb):
        e = nb - 1 - b
        PF[0, b] = fwd.astype(bf16)
        PF[1, e] = bwd.astype(bf16)
        fwd = jnp.exp(TD[0, b]) * fwd + U[0, b]
        bwd = jnp.exp(TD[1, e]) * bwd + U[1, e]
    LM[...] = message(fwd, bwd)
    for i in far_first(nz):
        push(LM.at[at_z(i)], LR.at[z], once_s.at[LMS], once_r.at[LMS], sp=at_z(i))
    sent(LMS, LM.at[pl.ds(0, nz - 1)])
    LR[z] = LM[z]

    def inner(b, carry):
        rows = pl.ds(al(b * BLOCK, BLOCK), BLOCK)
        total = O[rows, :]
        for d in range(2):
            cols = slice(d * DK, (d + 1) * DK)
            q_in = QF[rows, cols]
            total = total + dot(q_in, PF[d, b], NT)
            QD[rows, cols] = (q_in.astype(f32) * jnp.exp(OFF[d, b])).astype(bf16)
        O[rows, :] = total
        return carry

    lax.fori_loop(0, nb, inner, 0)

    all_in(CMS, CR.at[pl.ds(0, nz - 1)])
    all_in(DMS, DR.at[pl.ds(0, nz - 1)])
    all_in(LMS, LR.at[pl.ds(0, nz - 1)])

    def context_chain(s, carry):
        fwd, bwd = carry
        e = nz - 1 - s
        fwd = jnp.exp(DR[s, 2:3]) * fwd + CR[s].astype(f32)[:dvs]
        bwd = jnp.exp(DR[e, 3:4]) * bwd + CR[e].astype(f32)[dvs:]
        return fwd, bwd

    slice0 = jnp.zeros((dvs, DK), f32)
    fwd, bwd = lax.fori_loop(0, nz, context_chain, (slice0, slice0))
    fwd_in, bwd_in = [], [None] * nz
    for s in range(nz):
        e = nz - 1 - s
        fwd_in.append(fwd)
        bwd_in[e] = bwd
        fwd = jnp.exp(DR[s, 0:1]) * fwd + LR[s].astype(f32)[:dvs]
        bwd = jnp.exp(DR[e, 1:2]) * bwd + LR[e].astype(f32)[dvs:]
    for s in range(nz):
        RO[s] = jnp.concatenate([fwd_in[s], bwd_in[s]], axis=0).astype(bf16)
    for i in far_first(nz):
        push(RO.at[at_z(i)], RR.at[z], once_s.at[ROS], once_r.at[ROS], sp=at_z(i))
    sent(ROS, RO.at[pl.ds(0, nz - 1)])
    RR[z] = RO[z]
    gate_rows = silu(PVG[:, VC:].astype(f32)) * gain[:, pl.ds(al(p * VC, VC), VC)]
    all_in(ROS, RR.at[pl.ds(0, nz - 1)])
    back = RR[...].astype(f32)
    start = jnp.concatenate(
        [back[:, :dvs].reshape(VC, DK), back[:, dvs:].reshape(VC, DK)], axis=1
    ).astype(bf16)
    mixture = O[...] + dot(QD[...], start, NT)

    SS[p] = dot(jnp.ones((8, VC), f32), mixture * mixture, NT, precision=highest)
    for i in range(1, share):
        push(
            SS.at[p],
            SS.at[p],
            once_s.at[SSS],
            once_r.at[SSS],
            tp=h * share + lax.rem(p + i, share),
        )
    sent(SSS, SS.at[pl.ds(0, share - 1)])
    GT[...] = (mixture * gate_rows).reshape(nt, TB, VC)

    def owner(q, j):
        chip = jnp.where(q // 2 == 0, 2 * h - j + nx, 2 * h + 1 + j)
        return lax.rem(chip, nx) * 2 + q % 2

    lanes = pl.ds(al(p * VC, VC), VC)
    for i in range(1, share):
        q = lax.rem(p + i, share)
        for j in range(heads):
            push(
                GT.at[owner(q, j)],
                GR.at[j, :, lanes],
                once_s.at[GRS],
                once_r.at[GRS],
                tp=h * share + q,
            )
    sent(GRS, GT.at[pl.ds(0, (share - 1) * heads)])
    for j in range(heads):
        GR[j, :, lanes] = GT[owner(p, j)]
    all_in(SSS, SS.at[pl.ds(0, share - 1)])
    squares = SS[0]
    for i in range(1, share):
        squares = squares + SS[i]
    IV[...] = lax.rsqrt(squares / (share * VC) + norm_eps).T.reshape(nt, TB, 8)
    all_in(WOUT, WO.at[pl.ds(0, (share - 1) * VC), :])
    all_in(GRS, GT.at[pl.ds(0, (share - 1) * heads)])

    left = jnp.concatenate(
        [(GR[j] * IV[owner(p, j)][:, 0:1]).astype(bf16) for j in range(heads)], axis=0
    )
    NC = D // 4
    for n in range(4):
        cols = slice(n * NC, (n + 1) * NC)
        partial = dot(left, WO[:, cols]).reshape(heads, TB, NC)
        ACC[:, cols] = partial[0]
        PS[:, :, cols] = partial.astype(bf16)
    for j in range(heads - 1, 0, -1):
        push(PS.at[j], PR.at[j], once_s.at[PRS], once_r.at[PRS], tp=owner(p, j))
    branch = ACC[...]
    if heads > 1:
        sent(PRS, PS.at[pl.ds(0, heads - 1)])
        all_in(PRS, PR.at[pl.ds(0, heads - 1)])
    for j in range(1, heads):
        branch = branch + PR[j].astype(f32)
    own = L[pl.ds(al(t * TB, TB), TB), :].astype(f32)
    gates = M[0:1, 2 * D :] + mod_b[:, 2 * D :]
    summed = residual_scale * own + gates * branch
    centered = summed - jnp.mean(summed, axis=1, keepdims=True)
    variance = jnp.mean(centered * centered, axis=1, keepdims=True)
    out[...] = (
        centered * lax.rsqrt(variance + norm_eps) * final_g[...] + final_b[...]
    ).astype(out.dtype)
    for copy in pending:
        copy.wait_send()

    @pl.when(core == 0)
    def _():
        waiter(L.at[pl.ds(0, 2 * (nx - 1) * TB), :], once_s.at[LX], once_r.at[LX]).wait_send()
        waiter(L.at[rest, :], once_s.at[LD], once_r.at[LD]).wait_send()

    @pl.when(core == 1)
    def _():
        view = W.at[pl.ds(0, (nz - 1) * KR), :]
        waiter(view, once_s.at[WZ], once_r.at[WZ]).wait_send()
        waiter(view, once_s.at[WD], once_r.at[WD]).wait_send()
        waiter(L.at[pl.ds(0, TB), :], once_s.at[LD], once_r.at[LD]).wait_send()


def body(
    nz,
    nt,
    latent,
    context,
    condition,
    context_condition,
    mod_weight,
    mod_bias,
    query_weight,
    key_weight,
    value_weight,
    out_gate_weight,
    decay_in_weight,
    decay_weight,
    decay_bias,
    extra_decay,
    norm_gain,
    out_weight,
    final_gain,
    final_bias,
):
    heads = ATTENTION_HEADS
    share = nt // heads
    D = latent.shape[1]
    TB = latent.shape[0]
    tok = TB * nt
    DK = query_weight.shape[1] // heads
    VC = value_weight.shape[1]
    MC = mod_weight.shape[1]
    nb = tok // BLOCK
    row_tab, col_tab = rotary_tables(nz * nb, DK // 2)
    dvs = VC // nz
    vmem = pl.BlockSpec(memory_space=pltpu.VMEM)
    hbm = pl.BlockSpec(memory_space=pl.ANY)
    dma = pltpu.SemaphoreType.DMA
    scratch = [
        pltpu.VMEM((tok, D), bf16),
        pltpu.VMEM((tok, D), bf16),
        pltpu.VMEM((D, 2 * DK), bf16),
        pltpu.VMEM((D, 2 * VC), bf16),
        pltpu.VMEM((share * VC, D), bf16),
        pltpu.VMEM((2, 3 * D), f32),
        pltpu.VMEM((nz, 2, MC), f32),
        pltpu.VMEM((tok, 2 * VC), bf16),
        pltpu.VMEM((tok, 2 * DK), bf16),
        pltpu.VMEM((tok, 2 * DK), bf16),
        pltpu.VMEM((tok, 2 * DK), bf16),
        pltpu.VMEM((tok, VC), f32),
        pltpu.VMEM((2, nb, VC, DK), f32),
        pltpu.VMEM((2, nb, 1, DK), f32),
        pltpu.VMEM((2, nb, VC, DK), bf16),
        pltpu.VMEM((2, nb, 1, DK), f32),
        pltpu.VMEM((nz, 2 * dvs, DK), bf16),
        pltpu.VMEM((nz, 2 * dvs, DK), bf16),
        pltpu.VMEM((nz, 2 * dvs, DK), bf16),
        pltpu.VMEM((nz, 2 * dvs, DK), bf16),
        pltpu.VMEM((4, DK), f32),
        pltpu.VMEM((nz, 4, DK), f32),
        pltpu.VMEM((nz, 2 * dvs, DK), bf16),
        pltpu.VMEM((nz, 2 * dvs, DK), bf16),
        pltpu.VMEM((share, 8, tok), f32),
        pltpu.VMEM((nt, TB, VC), f32),
        pltpu.VMEM((heads, TB, share * VC), f32),
        pltpu.VMEM((TB, D), f32),
        pltpu.VMEM((heads, TB, D), bf16),
        pltpu.VMEM((heads, TB, D), bf16),
        pltpu.VMEM((nt, TB, 8), f32),
        *[
            pltpu.VMEM(shape, kind)
            for shape, kind in (
                ((1, condition.shape[0]), f32),
                ((1, context_condition.shape[0]), f32),
                (mod_weight.shape, bf16),
                ((1, mod_bias.shape[0]), f32),
                (decay_weight.shape, bf16),
                (decay_bias.shape, f32),
                (extra_decay.shape, f32),
                ((1, norm_gain.shape[0]), f32),
                ((1, D), f32),
                ((1, D), f32),
            )
        ],
        pltpu.VMEM(context.shape, bf16),
        pltpu.VMEM((decay_in_weight.shape[1], D), bf16),
        pltpu.VMEM(row_tab.shape, f32),
        pltpu.VMEM(col_tab.shape, f32),
        pltpu.VMEM((2, tok, DK), f32),
        pltpu.VMEM((2, tok, DK), f32),
        pltpu.VMEM((2, tok, DK), f32),
        dma((20,)),
        dma((14,)),
        dma((14,)),
        dma((4 * (nz // 2),)),
        dma((4 * (nt // 4),)),
    ]
    in_specs = [hbm] * 20
    return pl.pallas_call(
        functools.partial(kernel, nz, nt, heads),
        out_shape=jax.ShapeDtypeStruct((TB, D), bf16),
        in_specs=in_specs,
        out_specs=vmem,
        scratch_shapes=scratch,
        compiler_params=pltpu.CompilerParams(
            collective_id=0, has_side_effects=True, vmem_limit_bytes=58 * 1024 * 1024
        ),
        name="layer",
    )(
        latent,
        context,
        condition.reshape(1, -1),
        context_condition.reshape(1, -1),
        mod_weight,
        mod_bias.reshape(1, -1),
        query_weight,
        key_weight,
        value_weight,
        out_gate_weight,
        decay_in_weight.T,
        decay_weight,
        decay_bias,
        extra_decay,
        norm_gain.reshape(1, -1),
        out_weight,
        final_gain.reshape(1, -1),
        final_bias.reshape(1, -1),
        jnp.asarray(row_tab),
        jnp.asarray(col_tab),
    )


def solution(mesh):
    placed = (
        P(("grp", "sp", "tp"), None),
        P(("grp", "sp"), None),
        P(("grp", "sp")),
        P("sp"),
        P("sp", "tp"),
        P(),
        P("sp", None),
        P("sp", None),
        P(None, "tp"),
        P(None, "tp"),
        P(),
        P(),
        P(),
        P(None, None, "sp"),
        P(),
        P("tp", None),
        P(),
        P(),
    )
    return jax.shard_map(
        functools.partial(body, mesh.shape["sp"], mesh.shape["tp"]),
        mesh=mesh,
        in_specs=placed,
        out_specs=P(("grp", "sp", "tp"), None),
        check_vma=False,
    )
```

```python
import functools

import numpy as np
import jax
import jax.numpy as jnp
from jax import lax
from jax.experimental import pallas as pl
from jax.experimental.pallas import tpu as pltpu
from jax.sharding import PartitionSpec as P

ATTENTION_HEADS = 4
DV = 512
BLOCK = 64
GRID_W = 64

norm_eps = 1e-05
gate_scale = 16.0
rope_base = 10000.0
residual_scale = 2.0**0.5
highest = lax.Precision.HIGHEST
f32 = jnp.float32
bf16 = jnp.bfloat16

NT = (((1,), (1,)), ((), ()))
TN = (((0,), (0,)), ((), ()))


def dot(a, b, dims=None, precision=None):
    if dims is None:
        dims = (((1,), (0,)), ((), ()))
    return lax.dot_general(a, b, dims, precision=precision, preferred_element_type=f32)


def log_sigmoid(v):
    return jnp.minimum(v, 0.0) - jnp.log1p(jnp.exp(-jnp.abs(v)))


def silu(v):
    return v / (1.0 + jnp.exp(-v))


def rotary_tables(rows, half):
    quarter = half // 2
    frequency = (rope_base ** (-np.arange(quarter, dtype=np.float64) / quarter)).astype(np.float32)

    def table(places):
        angle = (np.arange(places, dtype=np.float32)[:, None] * frequency).astype(np.float64)
        cosine = np.cos(angle)
        sine = np.sin(angle)
        return np.stack(
            [np.concatenate([cosine, cosine], 1), np.concatenate([-sine, sine], 1)]
        ).astype(np.float32)

    return table(rows), table(GRID_W)


def spread(n, j):
    long, short = n // 2, (n - 1) // 2
    right, left = (long, short) if j % 2 == 0 else (short, long)
    steps = {a: [a + 1] for a in range(1, right)} | {-a: [-a - 1] for a in range(1, left)}
    steps[0] = ([1] if right else []) + ([-1] if left else [])
    due = [o for a in range(1, long + 1) for o in (a, -a) if o <= right and o >= -left]
    return due, steps


def kernel(
    nz,
    nt,
    heads,
    lat_in,
    ctx_hbm,
    cond_hbm,
    ctx_cond_hbm,
    mod_w_hbm,
    mod_b_hbm,
    qw,
    kw,
    vw,
    gw,
    low_hbm,
    decay_w_hbm,
    decay_b_hbm,
    extra_hbm,
    gain_hbm,
    out_w,
    final_g_hbm,
    final_b_hbm,
    row_hbm,
    col_hbm,
    out,
    L,
    XM,
    W,
    VG,
    WO,
    M,
    mod_part,
    PVG,
    PLOW,
    PQK,
    QF,
    QD,
    O,
    U,
    TD,
    PF,
    OFF,
    LM,
    LR,
    CM,
    CR,
    DM,
    DR,
    RO,
    RR,
    SS,
    GT,
    GR,
    ACC,
    PS,
    PR,
    IV,
    cond,
    ctx_cond,
    mod_w,
    mod_b,
    decay_w,
    decay_b,
    extra,
    gain,
    final_g,
    final_b,
    CX,
    LOWT,
    RT,
    CT,
    EC,
    EI,
    EO,
    loc_sem,
    once_s,
    once_r,
    wz_r,
    lx_r,
):
    z = lax.axis_index("sp")
    t = lax.axis_index("tp")
    share = nt // heads
    h = t // share
    p = t % share
    core = t % 2
    x = t // 2
    nx = nt // 2
    partner = t + 1 - 2 * core
    D = lat_in.shape[1]
    TB = lat_in.shape[0]
    tok = TB * nt
    KR = qw.shape[0]
    DK = qw.shape[1] // heads
    HC = DK // 2
    VC = vw.shape[1]
    MC = mod_w_hbm.shape[1]
    nb = tok // BLOCK
    dvs = VC // nz
    pending = []
    MP, MG, WZ, WD, LX, LD, WOUT, LMS, CMS, DMS, ROS, SSS, GRS, PRS = range(14)

    def push(src, dst, ssem, rsem, **where):
        pltpu.make_async_remote_copy(
            src_ref=src,
            dst_ref=dst,
            send_sem=ssem,
            recv_sem=rsem,
            device_id=where,
            device_id_type=pl.DeviceIdType.MESH,
        ).start()

    def waiter(view, ssem, rsem):
        return pltpu.make_async_remote_copy(
            src_ref=view,
            dst_ref=view,
            send_sem=ssem,
            recv_sem=rsem,
            device_id={"tp": partner},
            device_id_type=pl.DeviceIdType.MESH,
        )

    def all_in(kind, view):
        waiter(view, once_s.at[kind], once_r.at[kind]).wait_recv()

    def sent(kind, view):
        pending.append(waiter(view, once_s.at[kind], once_r.at[kind]))

    def far_first(n):
        return sorted(range(1, n), key=lambda i: (-min(i, n - i), i))

    def at_z(i):
        return lax.rem(z + i + nz, nz)

    def at_t(i):
        return lax.rem(t + i + nt, nt)

    def at_x(i):
        return lax.rem(x + i + nx, nx)

    def al(v, m):
        return pl.multiple_of(v, m)

    def w_at(zz, j, parts=2):
        rows = KR // parts
        first = zz * KR + (j % parts) * rows
        return W.at[pl.ds(al(first, rows), rows), pl.ds((j // parts) * DK, DK)]

    def l_at(xx, j):
        rows = pl.ds(al((xx * 2 + j // 2) * TB, TB), TB)
        return L.at[rows, pl.ds((j % 2) * (D // 2), D // 2)]

    head_cols = pl.ds(al(h * DK, DK), DK)
    loads = [
        (cond_hbm, cond),
        (ctx_cond_hbm, ctx_cond),
        (mod_w_hbm, mod_w),
        (lat_in, L.at[pl.ds(al(t * TB, TB), TB), :]),
        (qw.at[:, head_cols], w_at(z, 0, 1)),
        (kw.at[:, head_cols], w_at(z, 1, 1)),
        (out_w, WO.at[pl.ds(al(p * VC, VC), VC), :]),
        (vw, VG.at[:, pl.ds(0, VC)]),
        (gw, VG.at[:, pl.ds(VC, VC)]),
        (ctx_hbm, CX),
        (low_hbm, LOWT),
        (mod_b_hbm, mod_b),
        (decay_w_hbm, decay_w),
        (decay_b_hbm, decay_b),
        (extra_hbm, extra),
        (gain_hbm, gain),
        (final_g_hbm, final_g),
        (final_b_hbm, final_b),
        (row_hbm, RT),
        (col_hbm, CT),
    ]
    local = [
        pltpu.make_async_copy(src, dst, loc_sem.at[i]) for i, (src, dst) in enumerate(loads)
    ]
    barrier = pltpu.get_barrier_semaphore()
    for i in far_first(nz):
        pl.semaphore_signal(
            barrier, inc=1, device_id={"sp": at_z(i)}, device_id_type=pl.DeviceIdType.MESH
        )
    for i in far_first(nt):
        pl.semaphore_signal(
            barrier, inc=1, device_id={"tp": at_t(i)}, device_id_type=pl.DeviceIdType.MESH
        )
    for copy in local:
        copy.start()
    for copy in local[:3]:
        copy.wait()

    both = jnp.concatenate([cond[...], ctx_cond[...], jnp.zeros((6, cond.shape[1]), f32)], axis=0)
    part = dot(silu(both).astype(bf16), mod_w[...])
    mod_part[z] = part[0:2]

    for copy in local[3:6]:
        copy.wait()
    pl.semaphore_wait(barrier, nz - 1 + nt - 1)

    for i in far_first(nz):
        push(mod_part.at[z], mod_part.at[z], once_s.at[MP], once_r.at[MP], sp=at_z(i))
    sent(MP, mod_part.at[pl.ds(0, nz - 1)])

    def ring(n, chunks, at, region, far, sem_r, kind, share_kind):
        plans = [spread(n, j) for j in range(chunks)]

        def give(o, j):
            src = region(at(-o), j)
            push(src, src, once_s.at[share_kind], once_r.at[share_kind], tp=partner)

        def hand_on(o, j):
            src = region(at(-o), j)
            for c in plans[j][1].get(o, []):
                sem = sem_r.at[(c % n) * chunks + j]
                push(src, src, once_s.at[kind], sem, **far(c - o))

        def take(first, last):
            for i in range(first, min(last, n - 1)):
                for j in range(chunks):
                    o = plans[j][0][i]
                    sem = sem_r.at[(o % n) * chunks + j]
                    waiter(region(at(-o), j), once_s.at[kind], sem).wait_recv()
                    hand_on(o, j)
                for j in range(chunks):
                    give(plans[j][0][i], j)

        return give, hand_on, take

    l_give, l_on, l_take = ring(
        nx, 4, at_x, l_at, lambda i: {"tp": at_x(i) * 2 + core}, lx_r, LX, LD
    )
    w_give, w_on, w_take = ring(nz, 4, at_z, w_at, lambda i: {"sp": at_z(i)}, wz_r, WZ, WD)
    rest = pl.ds(0, (2 * nx - 1) * TB)

    @pl.when(core == 0)
    def _():
        for j in range(2):
            l_on(0, j)
        for j in range(2):
            l_give(0, j)
        all_in(LD, L.at[pl.ds(0, TB), :])
        for j in range(2, 4):
            l_on(0, j)
        l_take(0, 4)

    @pl.when(core == 1)
    def _():
        for j in range(2, 4):
            l_give(0, j)
        for j in range(4):
            w_on(0, j)
        w_take(0, 6)

    def modulation_sums():
        all_in(MP, mod_part.at[pl.ds(0, nz - 1)])
        sums = mod_part[0]
        for i in range(1, nz):
            sums = sums + mod_part[i]
        cols = pl.ds(al(t * MC, 128), MC)
        M[:, cols] = sums
        for i in far_first(nt):
            push(M.at[:, cols], M.at[:, cols], once_s.at[MG], once_r.at[MG], tp=at_t(i))
        sent(MG, M.at[:, pl.ds(0, (nt - 1) * MC)])

    modulation_sums()

    @pl.when(core == 0)
    def _():
        l_take(4, nx - 1)

    @pl.when(core == 1)
    def _():
        w_take(6, 12)

    local[6].wait()
    own_rows = WO.at[pl.ds(al(p * VC, VC), VC), :]
    for i in range(1, share):
        push(
            own_rows,
            own_rows,
            once_s.at[WOUT],
            once_r.at[WOUT],
            tp=h * share + lax.rem(p + i, share),
        )
    sent(WOUT, WO.at[pl.ds(0, (share - 1) * VC), :])
    all_in(MG, M.at[:, pl.ds(0, (nt - 1) * MC)])
    for copy in local[7:]:
        copy.wait()

    mod = M[...] + mod_b[...]
    shift, scale = mod[:, :D], 1.0 + mod[:, D : 2 * D]
    bias = decay_b[:, pl.ds(al(h * DK, DK), DK)]
    rank = decay_w.shape[1]
    zero = jnp.zeros((rank, DK), bf16)
    maps = [
        jnp.concatenate([decay_w[0, :, head_cols], zero], axis=0),
        jnp.concatenate([zero, decay_w[1, :, head_cols]], axis=0),
    ]

    def triangles(size):
        row = lax.broadcasted_iota(jnp.int32, (size, size), 0)
        col = lax.broadcasted_iota(jnp.int32, (size, size), 1)
        return row >= col, row <= col

    low_b, up_b = triangles(BLOCK)
    added = [extra[d, pl.ds(h, 1), :] for d in range(2)]

    def decays(low, d):
        return log_sigmoid(dot(low, maps[d]) + bias[d : d + 1]) * (1.0 / gate_scale)

    @pl.when(core == 1)
    def _():
        all_in(LD, L.at[rest, :])

    def context_decays():
        ctx_rows = (CX[...].astype(f32) * scale[1:2] + shift[1:2]).astype(bf16)
        ctx_values = dot(ctx_rows, VG[:, 0:VC]).astype(bf16)
        ctx_low = dot(ctx_rows, LOWT[...], NT).astype(bf16)
        CB = ctx_hbm.shape[0]
        low_c, up_c = triangles(CB)
        cum_f = dot(low_c.astype(f32), decays(ctx_low, 0), precision=highest)
        cum_b = dot(up_c.astype(f32), decays(ctx_low, 1), precision=highest)
        tot_cf, tot_cb = cum_f[CB - 1 : CB], cum_b[0:1]
        return ctx_rows, ctx_values, cum_f, cum_b, tot_cf, tot_cb

    tiles = max(1, tok // 128)
    TR = tok // tiles

    def values_tile(i):
        rows = pl.ds(i * TR, TR)
        rounded = (L[rows, :].astype(f32) * scale[0:1] + shift[0:1]).astype(bf16)
        XM[rows, :] = rounded
        PVG[rows, :] = dot(rounded, VG[...]).astype(bf16)
        PLOW[rows, :] = dot(rounded, LOWT[...], NT).astype(bf16)

    def decays_tile(i):
        low = PLOW[pl.ds(i * TR, TR), :]
        for d, mask in ((0, low_b), (1, up_b)):
            steps = decays(low, d)
            for b in range(i * TR // BLOCK, (i + 1) * TR // BLOCK):
                at = b * BLOCK - i * TR
                ex = added[d][:, b * BLOCK : (b + 1) * BLOCK]
                cum = dot(mask.astype(f32), steps[at : at + BLOCK], precision=highest) + jnp.sum(
                    jnp.where(mask, ex, 0.0), axis=1, keepdims=True
                )
                total = cum[BLOCK - 1 : BLOCK] if d == 0 else cum[0:1]
                block_rows = slice(b * BLOCK, (b + 1) * BLOCK)
                EC[d, block_rows, :] = jnp.exp(cum)
                EI[d, block_rows, :] = jnp.exp(-cum)
                EO[d, block_rows, :] = jnp.exp(total - cum)
                TD[d, b] = total

    pieces = [f for i in range(tiles) for f in ((values_tile, i), (decays_tile, i))]
    for n, (piece, i) in enumerate(pieces):
        piece(i)
        if n < 3:
            first, last = 12 + n, (13 + n if n + 1 < min(3, len(pieces)) else nz - 1)

            @pl.when(core == 1)
            def _():
                w_take(first, last)

    ctx_rows, ctx_values, cum_f, cum_b, tot_cf, tot_cb = context_decays()
    sum_f, sum_b = jnp.zeros((1, DK), f32), jnp.zeros((1, DK), f32)
    for b in range(nb):
        OFF[0, b] = sum_f
        OFF[1, nb - 1 - b] = sum_b
        sum_f = sum_f + TD[0, b]
        sum_b = sum_b + TD[1, nb - 1 - b]
    DM[...] = jnp.concatenate([sum_f, sum_b, tot_cf, tot_cb], axis=0)
    for i in far_first(nz):
        push(DM, DR.at[z], once_s.at[DMS], once_r.at[DMS], sp=at_z(i))
    sent(DMS, DR.at[pl.ds(0, nz - 1)])
    DR[z] = DM[...]

    def message(forward, backward):
        return jnp.concatenate(
            [forward.reshape(nz, dvs, DK), backward.reshape(nz, dvs, DK)], axis=1
        ).astype(bf16)

    @pl.when(core == 0)
    def _():
        all_in(WD, W.at[pl.ds(0, (nz - 1) * KR), :])

    ctx_keys = dot(ctx_rows, W[:, DK : 2 * DK]).astype(bf16).astype(f32)
    CM[...] = message(
        dot(ctx_values, (ctx_keys * jnp.exp(tot_cf - cum_f)).astype(bf16), TN),
        dot(ctx_values, (ctx_keys * jnp.exp(tot_cb - cum_b)).astype(bf16), TN),
    )
    for i in far_first(nz):
        push(CM.at[at_z(i)], CR.at[z], once_s.at[CMS], once_r.at[CMS], sp=at_z(i))
    sent(CMS, CM.at[pl.ds(0, nz - 1)])
    CR[z] = CM[z]

    QT = min(tok, 256)

    def project_qk(i, carry):
        rows = pl.ds(al(i * QT, QT), QT)
        PQK[rows, :] = dot(XM[rows, :], W[...]).astype(bf16)
        return carry

    lax.fori_loop(0, tok // QT, project_qk, 0)

    half = DK // 2
    for b in range(nb):
        rows = slice(b * BLOCK, (b + 1) * BLOCK)
        place = pl.ds(z * nb + b, 1)
        row_cos, row_sin = RT[0, place, :], RT[1, place, :]

        def rotated(values):
            first, second = values[:, :half], values[:, half:]
            return jnp.concatenate(
                [
                    first * row_cos + pltpu.roll(first, half // 2, 1) * row_sin,
                    second * CT[0] + pltpu.roll(second, half // 2, 1) * CT[1],
                ],
                axis=1,
            )

        q = rotated(PQK[rows, :DK].astype(f32)) * DK ** (-0.5)
        k = rotated(PQK[rows, DK:].astype(f32))
        v = PVG[rows, 0:VC]
        scores = None
        for d, mask in ((0, low_b), (1, up_b)):
            q_in = (q * EC[d, rows, :]).astype(bf16)
            k_in = (k * EI[d, rows, :]).astype(bf16)
            k_out = (k * EO[d, rows, :]).astype(bf16)
            QF[rows, d * DK : (d + 1) * DK] = q_in
            U[d, b] = dot(v, k_out, TN)
            one = jnp.where(mask, dot(q_in, k_in, NT), 0.0)
            scores = one if scores is None else scores + one
        O[rows, :] = dot(scores.astype(bf16), v)

    fwd, bwd = jnp.zeros((VC, DK), f32), jnp.zeros((VC, DK), f32)
    for b in range(nb):
        e = nb - 1 - b
        PF[0, b] = fwd.astype(bf16)
        PF[1, e] = bwd.astype(bf16)
        fwd = jnp.exp(TD[0, b]) * fwd + U[0, b]
        bwd = jnp.exp(TD[1, e]) * bwd + U[1, e]
    LM[...] = message(fwd, bwd)
    for i in far_first(nz):
        push(LM.at[at_z(i)], LR.at[z], once_s.at[LMS], once_r.at[LMS], sp=at_z(i))
    sent(LMS, LM.at[pl.ds(0, nz - 1)])
    LR[z] = LM[z]

    def inner(b, carry):
        rows = pl.ds(al(b * BLOCK, BLOCK), BLOCK)
        total = O[rows, :]
        for d in range(2):
            cols = slice(d * DK, (d + 1) * DK)
            q_in = QF[rows, cols]
            total = total + dot(q_in, PF[d, b], NT)
            QD[rows, cols] = (q_in.astype(f32) * jnp.exp(OFF[d, b])).astype(bf16)
        O[rows, :] = total
        return carry

    lax.fori_loop(0, nb, inner, 0)

    all_in(CMS, CR.at[pl.ds(0, nz - 1)])
    all_in(DMS, DR.at[pl.ds(0, nz - 1)])
    all_in(LMS, LR.at[pl.ds(0, nz - 1)])

    def context_chain(s, carry):
        fwd, bwd = carry
        e = nz - 1 - s
        fwd = jnp.exp(DR[s, 2:3]) * fwd + CR[s].astype(f32)[:dvs]
        bwd = jnp.exp(DR[e, 3:4]) * bwd + CR[e].astype(f32)[dvs:]
        return fwd, bwd

    slice0 = jnp.zeros((dvs, DK), f32)
    fwd, bwd = lax.fori_loop(0, nz, context_chain, (slice0, slice0))
    fwd_in, bwd_in = [], [None] * nz
    for s in range(nz):
        e = nz - 1 - s
        fwd_in.append(fwd)
        bwd_in[e] = bwd
        fwd = jnp.exp(DR[s, 0:1]) * fwd + LR[s].astype(f32)[:dvs]
        bwd = jnp.exp(DR[e, 1:2]) * bwd + LR[e].astype(f32)[dvs:]
    for s in range(nz):
        RO[s] = jnp.concatenate([fwd_in[s], bwd_in[s]], axis=0).astype(bf16)
    for i in far_first(nz):
        push(RO.at[at_z(i)], RR.at[z], once_s.at[ROS], once_r.at[ROS], sp=at_z(i))
    sent(ROS, RO.at[pl.ds(0, nz - 1)])
    RR[z] = RO[z]
    gate_rows = silu(PVG[:, VC:].astype(f32)) * gain[:, pl.ds(al(p * VC, VC), VC)]
    all_in(ROS, RR.at[pl.ds(0, nz - 1)])
    back = RR[...].astype(f32)
    start = jnp.concatenate(
        [back[:, :dvs].reshape(VC, DK), back[:, dvs:].reshape(VC, DK)], axis=1
    ).astype(bf16)
    mixture = O[...] + dot(QD[...], start, NT)

    SS[p] = dot(jnp.ones((8, VC), f32), mixture * mixture, NT, precision=highest)
    for i in range(1, share):
        push(
            SS.at[p],
            SS.at[p],
            once_s.at[SSS],
            once_r.at[SSS],
            tp=h * share + lax.rem(p + i, share),
        )
    sent(SSS, SS.at[pl.ds(0, share - 1)])
    GT[...] = (mixture * gate_rows).reshape(nt, TB, VC)

    def owner(q, j):
        chip = jnp.where(q // 2 == 0, 2 * h - j + nx, 2 * h + 1 + j)
        return lax.rem(chip, nx) * 2 + q % 2

    lanes = pl.ds(al(p * VC, VC), VC)
    for i in range(1, share):
        q = lax.rem(p + i, share)
        for j in range(heads):
            push(
                GT.at[owner(q, j)],
                GR.at[j, :, lanes],
                once_s.at[GRS],
                once_r.at[GRS],
                tp=h * share + q,
            )
    sent(GRS, GT.at[pl.ds(0, (share - 1) * heads)])
    for j in range(heads):
        GR[j, :, lanes] = GT[owner(p, j)]
    all_in(SSS, SS.at[pl.ds(0, share - 1)])
    squares = SS[0]
    for i in range(1, share):
        squares = squares + SS[i]
    IV[...] = lax.rsqrt(squares / (share * VC) + norm_eps).T.reshape(nt, TB, 8)
    all_in(WOUT, WO.at[pl.ds(0, (share - 1) * VC), :])
    all_in(GRS, GT.at[pl.ds(0, (share - 1) * heads)])

    left = jnp.concatenate(
        [(GR[j] * IV[owner(p, j)][:, 0:1]).astype(bf16) for j in range(heads)], axis=0
    )
    NC = D // 4
    for n in range(4):
        cols = slice(n * NC, (n + 1) * NC)
        partial = dot(left, WO[:, cols]).reshape(heads, TB, NC)
        ACC[:, cols] = partial[0]
        PS[:, :, cols] = partial.astype(bf16)
    for j in range(heads - 1, 0, -1):
        push(PS.at[j], PR.at[j], once_s.at[PRS], once_r.at[PRS], tp=owner(p, j))
    branch = ACC[...]
    if heads > 1:
        sent(PRS, PS.at[pl.ds(0, heads - 1)])
        all_in(PRS, PR.at[pl.ds(0, heads - 1)])
    for j in range(1, heads):
        branch = branch + PR[j].astype(f32)
    own = L[pl.ds(al(t * TB, TB), TB), :].astype(f32)
    gates = M[0:1, 2 * D :] + mod_b[:, 2 * D :]
    summed = residual_scale * own + gates * branch
    centered = summed - jnp.mean(summed, axis=1, keepdims=True)
    variance = jnp.mean(centered * centered, axis=1, keepdims=True)
    out[...] = (
        centered * lax.rsqrt(variance + norm_eps) * final_g[...] + final_b[...]
    ).astype(out.dtype)
    for copy in pending:
        copy.wait_send()

    @pl.when(core == 0)
    def _():
        waiter(L.at[pl.ds(0, 2 * (nx - 1) * TB), :], once_s.at[LX], once_r.at[LX]).wait_send()
        waiter(L.at[rest, :], once_s.at[LD], once_r.at[LD]).wait_send()

    @pl.when(core == 1)
    def _():
        view = W.at[pl.ds(0, (nz - 1) * KR), :]
        waiter(view, once_s.at[WZ], once_r.at[WZ]).wait_send()
        waiter(view, once_s.at[WD], once_r.at[WD]).wait_send()
        waiter(L.at[pl.ds(0, TB), :], once_s.at[LD], once_r.at[LD]).wait_send()


def body(
    nz,
    nt,
    latent,
    context,
    condition,
    context_condition,
    mod_weight,
    mod_bias,
    query_weight,
    key_weight,
    value_weight,
    out_gate_weight,
    decay_in_weight,
    decay_weight,
    decay_bias,
    extra_decay,
    norm_gain,
    out_weight,
    final_gain,
    final_bias,
):
    heads = ATTENTION_HEADS
    share = nt // heads
    D = latent.shape[1]
    TB = latent.shape[0]
    tok = TB * nt
    DK = query_weight.shape[1] // heads
    VC = value_weight.shape[1]
    MC = mod_weight.shape[1]
    nb = tok // BLOCK
    row_tab, col_tab = rotary_tables(nz * nb, DK // 2)
    dvs = VC // nz
    vmem = pl.BlockSpec(memory_space=pltpu.VMEM)
    hbm = pl.BlockSpec(memory_space=pl.ANY)
    dma = pltpu.SemaphoreType.DMA
    scratch = [
        pltpu.VMEM((tok, D), bf16),
        pltpu.VMEM((tok, D), bf16),
        pltpu.VMEM((D, 2 * DK), bf16),
        pltpu.VMEM((D, 2 * VC), bf16),
        pltpu.VMEM((share * VC, D), bf16),
        pltpu.VMEM((2, 3 * D), f32),
        pltpu.VMEM((nz, 2, MC), f32),
        pltpu.VMEM((tok, 2 * VC), bf16),
        pltpu.VMEM((tok, decay_in_weight.shape[1]), bf16),
        pltpu.VMEM((tok, 2 * DK), bf16),
        pltpu.VMEM((tok, 2 * DK), bf16),
        pltpu.VMEM((tok, 2 * DK), bf16),
        pltpu.VMEM((tok, VC), f32),
        pltpu.VMEM((2, nb, VC, DK), f32),
        pltpu.VMEM((2, nb, 1, DK), f32),
        pltpu.VMEM((2, nb, VC, DK), bf16),
        pltpu.VMEM((2, nb, 1, DK), f32),
        pltpu.VMEM((nz, 2 * dvs, DK), bf16),
        pltpu.VMEM((nz, 2 * dvs, DK), bf16),
        pltpu.VMEM((nz, 2 * dvs, DK), bf16),
        pltpu.VMEM((nz, 2 * dvs, DK), bf16),
        pltpu.VMEM((4, DK), f32),
        pltpu.VMEM((nz, 4, DK), f32),
        pltpu.VMEM((nz, 2 * dvs, DK), bf16),
        pltpu.VMEM((nz, 2 * dvs, DK), bf16),
        pltpu.VMEM((share, 8, tok), f32),
        pltpu.VMEM((nt, TB, VC), f32),
        pltpu.VMEM((heads, TB, share * VC), f32),
        pltpu.VMEM((TB, D), f32),
        pltpu.VMEM((heads, TB, D), bf16),
        pltpu.VMEM((heads, TB, D), bf16),
        pltpu.VMEM((nt, TB, 8), f32),
        *[
            pltpu.VMEM(shape, kind)
            for shape, kind in (
                ((1, condition.shape[0]), f32),
                ((1, context_condition.shape[0]), f32),
                (mod_weight.shape, bf16),
                ((1, mod_bias.shape[0]), f32),
                (decay_weight.shape, bf16),
                (decay_bias.shape, f32),
                (extra_decay.shape, f32),
                ((1, norm_gain.shape[0]), f32),
                ((1, D), f32),
                ((1, D), f32),
            )
        ],
        pltpu.VMEM(context.shape, bf16),
        pltpu.VMEM((decay_in_weight.shape[1], D), bf16),
        pltpu.VMEM(row_tab.shape, f32),
        pltpu.VMEM(col_tab.shape, f32),
        pltpu.VMEM((2, tok, DK), f32),
        pltpu.VMEM((2, tok, DK), f32),
        pltpu.VMEM((2, tok, DK), f32),
        dma((20,)),
        dma((14,)),
        dma((14,)),
        dma((4 * nz,)),
        dma((2 * nt,)),
    ]
    in_specs = [hbm] * 20
    return pl.pallas_call(
        functools.partial(kernel, nz, nt, heads),
        out_shape=jax.ShapeDtypeStruct((TB, D), bf16),
        in_specs=in_specs,
        out_specs=vmem,
        scratch_shapes=scratch,
        compiler_params=pltpu.CompilerParams(
            collective_id=0, has_side_effects=True, vmem_limit_bytes=58 * 1024 * 1024
        ),
        name="layer",
    )(
        latent,
        context,
        condition.reshape(1, -1),
        context_condition.reshape(1, -1),
        mod_weight,
        mod_bias.reshape(1, -1),
        query_weight,
        key_weight,
        value_weight,
        out_gate_weight,
        decay_in_weight.T,
        decay_weight,
        decay_bias,
        extra_decay,
        norm_gain.reshape(1, -1),
        out_weight,
        final_gain.reshape(1, -1),
        final_bias.reshape(1, -1),
        jnp.asarray(row_tab),
        jnp.asarray(col_tab),
    )


def solution(mesh):
    placed = (
        P(("grp", "sp", "tp"), None),
        P(("grp", "sp"), None),
        P(("grp", "sp")),
        P("sp"),
        P("sp", "tp"),
        P(),
        P("sp", None),
        P("sp", None),
        P(None, "tp"),
        P(None, "tp"),
        P(),
        P(),
        P(),
        P(None, None, "sp"),
        P(),
        P("tp", None),
        P(),
        P(),
    )
    return jax.shard_map(
        functools.partial(body, mesh.shape["sp"], mesh.shape["tp"]),
        mesh=mesh,
        in_specs=placed,
        out_specs=P(("grp", "sp", "tp"), None),
        check_vma=False,
    )
```

```python
import functools

import numpy as np
import jax
import jax.numpy as jnp
from jax import lax
from jax.experimental import pallas as pl
from jax.experimental.pallas import tpu as pltpu
from jax.sharding import PartitionSpec as P

ATTENTION_HEADS = 4
DV = 512
BLOCK = 64
GRID_W = 64

norm_eps = 1e-05
gate_scale = 16.0
rope_base = 10000.0
residual_scale = 2.0**0.5
highest = lax.Precision.HIGHEST
f32 = jnp.float32
bf16 = jnp.bfloat16

NT = (((1,), (1,)), ((), ()))
TN = (((0,), (0,)), ((), ()))


def dot(a, b, dims=None, precision=None):
    if dims is None:
        dims = (((1,), (0,)), ((), ()))
    return lax.dot_general(a, b, dims, precision=precision, preferred_element_type=f32)


def halves(a):
    high = a.astype(bf16)
    return high, (a - high.astype(f32)).astype(bf16)


def dot2(a, b, dims=None):
    high, low = halves(b)
    return dot(a, high, dims) + dot(a, low, dims)


def dot3(a, b, dims=None):
    a_high, a_low = halves(a)
    b_high, b_low = halves(b)
    return dot(a_high, b_high, dims) + (dot(a_high, b_low, dims) + dot(a_low, b_high, dims))


def log_sigmoid(v):
    return jnp.minimum(v, 0.0) - jnp.log1p(jnp.exp(-jnp.abs(v)))


def silu(v):
    return v / (1.0 + jnp.exp(-v))


def rotary_tables(rows, half):
    quarter = half // 2
    frequency = (rope_base ** (-np.arange(quarter, dtype=np.float64) / quarter)).astype(np.float32)

    def table(places):
        angle = (np.arange(places, dtype=np.float32)[:, None] * frequency).astype(np.float64)
        cosine = np.cos(angle)
        sine = np.sin(angle)
        return np.stack(
            [np.concatenate([cosine, cosine], 1), np.concatenate([-sine, sine], 1)]
        ).astype(np.float32)

    return table(rows), table(GRID_W)


def spread(n, j):
    long, short = n // 2, (n - 1) // 2
    right, left = (long, short) if j % 2 == 0 else (short, long)
    steps = {a: [a + 1] for a in range(1, right)} | {-a: [-a - 1] for a in range(1, left)}
    steps[0] = ([1] if right else []) + ([-1] if left else [])
    due = [o for a in range(1, long + 1) for o in (a, -a) if o <= right and o >= -left]
    return due, steps


def kernel(
    nz,
    nt,
    heads,
    lat_in,
    ctx_hbm,
    cond_hbm,
    ctx_cond_hbm,
    mod_w_hbm,
    mod_b_hbm,
    qw,
    kw,
    vw,
    gw,
    low_hbm,
    decay_w_hbm,
    decay_b_hbm,
    extra_hbm,
    gain_hbm,
    out_w,
    final_g_hbm,
    final_b_hbm,
    row_hbm,
    col_hbm,
    out,
    L,
    XM,
    W,
    VG,
    WO,
    M,
    mod_part,
    PVG,
    PLOW,
    PQK,
    QK,
    QD,
    O,
    U,
    TD,
    PF,
    OFF,
    LM,
    LR,
    CM,
    CR,
    DM,
    DR,
    RO,
    RR,
    SS,
    GT,
    GR,
    ACC,
    PS,
    PR,
    IV,
    cond,
    ctx_cond,
    mod_w,
    mod_b,
    decay_w,
    decay_b,
    extra,
    gain,
    final_g,
    final_b,
    CX,
    LOWT,
    RT,
    CT,
    EC,
    EI,
    EO,
    loc_sem,
    once_s,
    once_r,
    wz_r,
    lx_r,
):
    z = lax.axis_index("sp")
    t = lax.axis_index("tp")
    share = nt // heads
    h = t // share
    p = t % share
    core = t % 2
    x = t // 2
    nx = nt // 2
    partner = t + 1 - 2 * core
    D = lat_in.shape[1]
    TB = lat_in.shape[0]
    tok = TB * nt
    KR = qw.shape[0]
    DK = qw.shape[1] // heads
    HC = DK // 2
    VC = vw.shape[1]
    MC = mod_w_hbm.shape[1]
    nb = tok // BLOCK
    dvs = VC // nz
    pending = []
    MP, MG, WZ, WD, LX, LD, WOUT, LMS, CMS, DMS, ROS, SSS, GRS, PRS, DXS = range(15)

    def push(src, dst, ssem, rsem, **where):
        pltpu.make_async_remote_copy(
            src_ref=src,
            dst_ref=dst,
            send_sem=ssem,
            recv_sem=rsem,
            device_id=where,
            device_id_type=pl.DeviceIdType.MESH,
        ).start()

    def waiter(view, ssem, rsem):
        return pltpu.make_async_remote_copy(
            src_ref=view,
            dst_ref=view,
            send_sem=ssem,
            recv_sem=rsem,
            device_id={"tp": partner},
            device_id_type=pl.DeviceIdType.MESH,
        )

    def all_in(kind, view):
        waiter(view, once_s.at[kind], once_r.at[kind]).wait_recv()

    def sent(kind, view):
        pending.append(waiter(view, once_s.at[kind], once_r.at[kind]))

    def far_first(n):
        return sorted(range(1, n), key=lambda i: (-min(i, n - i), i))

    def at_z(i):
        return lax.rem(z + i + nz, nz)

    def at_t(i):
        return lax.rem(t + i + nt, nt)

    def at_x(i):
        return lax.rem(x + i + nx, nx)

    def al(v, m):
        return pl.multiple_of(v, m)

    def w_at(zz, j, parts=2):
        rows = KR // parts
        first = zz * KR + (j % parts) * rows
        return W.at[pl.ds(al(first, rows), rows), pl.ds((j // parts) * DK, DK)]

    def l_at(xx, j):
        rows = pl.ds(al((xx * 2 + j // 2) * TB, TB), TB)
        return L.at[rows, pl.ds((j % 2) * (D // 2), D // 2)]

    head_cols = pl.ds(al(h * DK, DK), DK)
    loads = [
        (cond_hbm, cond),
        (ctx_cond_hbm, ctx_cond),
        (mod_w_hbm, mod_w),
        (lat_in, L.at[pl.ds(al(t * TB, TB), TB), :]),
        (qw.at[:, head_cols], w_at(z, 0, 1)),
        (kw.at[:, head_cols], w_at(z, 1, 1)),
        (out_w, WO.at[pl.ds(al(p * VC, VC), VC), :]),
        (vw, VG.at[:, pl.ds(0, VC)]),
        (gw, VG.at[:, pl.ds(VC, VC)]),
        (ctx_hbm, CX),
        (low_hbm, LOWT),
        (mod_b_hbm, mod_b),
        (decay_w_hbm, decay_w),
        (decay_b_hbm, decay_b),
        (extra_hbm, extra),
        (gain_hbm, gain),
        (final_g_hbm, final_g),
        (final_b_hbm, final_b),
        (row_hbm, RT),
        (col_hbm, CT),
    ]
    local = [
        pltpu.make_async_copy(src, dst, loc_sem.at[i]) for i, (src, dst) in enumerate(loads)
    ]
    barrier = pltpu.get_barrier_semaphore()
    for i in far_first(nz):
        pl.semaphore_signal(
            barrier, inc=1, device_id={"sp": at_z(i)}, device_id_type=pl.DeviceIdType.MESH
        )
    for i in far_first(nt):
        pl.semaphore_signal(
            barrier, inc=1, device_id={"tp": at_t(i)}, device_id_type=pl.DeviceIdType.MESH
        )
    for copy in local[:6]:
        copy.start()
    for copy in local[:3]:
        copy.wait()

    both = jnp.concatenate([cond[...], ctx_cond[...], jnp.zeros((6, cond.shape[1]), f32)], axis=0)
    part = dot(silu(both).astype(bf16), mod_w[...])
    mod_part[z] = part[0:2]

    for copy in local[3:6]:
        copy.wait()
    pl.semaphore_wait(barrier, nz - 1 + nt - 1)

    for i in far_first(nz):
        push(mod_part.at[z], mod_part.at[z], once_s.at[MP], once_r.at[MP], sp=at_z(i))
    sent(MP, mod_part.at[pl.ds(0, nz - 1)])

    def ring(n, chunks, at, region, whole, far, sem_r, kind, share_kind):
        plans = [spread(n, j) for j in range(chunks)]

        def hand_on(o, j):
            src = region(at(-o), j)
            for c in plans[j][1].get(o, []):
                sem = sem_r.at[(c % n) * chunks + j]
                push(src, src, once_s.at[kind], sem, **far(c - o))

        def take(first, last):
            for i in range(first, min(last, n - 1)):
                for j in range(chunks):
                    o = plans[j][0][i]
                    sem = sem_r.at[(o % n) * chunks + j]
                    waiter(region(at(-o), j), once_s.at[kind], sem).wait_recv()
                    hand_on(o, j)
                src = whole(at(-plans[0][0][i]))
                push(src, src, once_s.at[share_kind], once_r.at[share_kind], tp=partner)

        return hand_on, take

    def l_whole(xx):
        return L.at[pl.ds(al(xx * 2 * TB, 2 * TB), 2 * TB), :]

    def w_whole(zz):
        return W.at[pl.ds(al(zz * KR, KR), KR), :]

    l_on, l_take = ring(
        nx, 4, at_x, l_at, l_whole, lambda i: {"tp": at_x(i) * 2 + core}, lx_r, LX, LD
    )
    w_on, w_take = ring(nz, 4, at_z, w_at, w_whole, lambda i: {"sp": at_z(i)}, wz_r, WZ, WD)
    own_rows = L.at[pl.ds(al(t * TB, TB), TB), :]
    rest = pl.ds(0, (2 * nx - 1) * TB)

    def load_rest():
        for copy in local[6:]:
            copy.start()

    @pl.when(core == 0)
    def _():
        for j in range(2):
            l_on(0, j)
        push(own_rows, own_rows, once_s.at[LD], once_r.at[LD], tp=partner)
        all_in(LD, L.at[pl.ds(0, TB), :])
        for j in range(2, 4):
            l_on(0, j)
        load_rest()
        l_take(0, 4)

    @pl.when(core == 1)
    def _():
        push(own_rows, own_rows, once_s.at[LD], once_r.at[LD], tp=partner)
        for j in range(4):
            w_on(0, j)
        load_rest()
        w_take(0, 6)

    def modulation_sums():
        all_in(MP, mod_part.at[pl.ds(0, nz - 1)])
        sums = mod_part[0]
        for i in range(1, nz):
            sums = sums + mod_part[i]
        cols = pl.ds(al(t * MC, 128), MC)
        M[:, cols] = sums
        for i in far_first(nt):
            push(M.at[:, cols], M.at[:, cols], once_s.at[MG], once_r.at[MG], tp=at_t(i))
        sent(MG, M.at[:, pl.ds(0, (nt - 1) * MC)])

    modulation_sums()

    @pl.when(core == 0)
    def _():
        l_take(4, nx - 1)

    @pl.when(core == 1)
    def _():
        w_take(6, 12)

    local[6].wait()
    proj_rows = WO.at[pl.ds(al(p * VC, VC), VC), :]
    for i in range(1, share):
        push(
            proj_rows,
            proj_rows,
            once_s.at[WOUT],
            once_r.at[WOUT],
            tp=h * share + lax.rem(p + i, share),
        )
    sent(WOUT, WO.at[pl.ds(0, (share - 1) * VC), :])
    all_in(MG, M.at[:, pl.ds(0, (nt - 1) * MC)])
    for copy in local[7:]:
        copy.wait()

    mod = M[...] + mod_b[...]
    shift, scale = mod[:, :D], 1.0 + mod[:, D : 2 * D]
    bias = decay_b[:, pl.ds(al(h * DK, DK), DK)]
    rank = decay_w.shape[1]
    zero = jnp.zeros((rank, DK), bf16)
    maps = [
        jnp.concatenate([decay_w[0, :, head_cols], zero], axis=0),
        jnp.concatenate([zero, decay_w[1, :, head_cols]], axis=0),
    ]

    def triangles(size):
        row = lax.broadcasted_iota(jnp.int32, (size, size), 0)
        col = lax.broadcasted_iota(jnp.int32, (size, size), 1)
        return row >= col, row <= col

    low_b, up_b = triangles(BLOCK)
    added = [extra[d, pl.ds(h, 1), :] for d in range(2)]

    def decays(low, d):
        return log_sigmoid(dot(low, maps[d]) + bias[d : d + 1]) * (1.0 / gate_scale)

    @pl.when(core == 1)
    def _():
        all_in(LD, L.at[rest, :])

    def message(forward, backward):
        return jnp.concatenate(
            [forward.reshape(nz, dvs, DK), backward.reshape(nz, dvs, DK)], axis=1
        ).astype(bf16)

    def context_states():
        ctx_rows = (CX[...].astype(f32) * scale[1:2] + shift[1:2]).astype(bf16)
        ctx_values = dot(ctx_rows, VG[:, 0:VC]).astype(bf16)
        ctx_low = dot(ctx_rows, LOWT[...], NT).astype(bf16)
        CB = ctx_hbm.shape[0]
        low_c, up_c = triangles(CB)
        cum_f = dot(low_c.astype(f32), decays(ctx_low, 0), precision=highest)
        cum_b = dot(up_c.astype(f32), decays(ctx_low, 1), precision=highest)
        tot_cf, tot_cb = cum_f[CB - 1 : CB], cum_b[0:1]
        DM[2] = tot_cf
        DM[3] = tot_cb
        ctx_keys = dot(ctx_rows, W[:, DK : 2 * DK]).astype(bf16).astype(f32)
        CM[...] = message(
            dot2(ctx_values, ctx_keys * jnp.exp(tot_cf - cum_f), TN),
            dot2(ctx_values, ctx_keys * jnp.exp(tot_cb - cum_b), TN),
        )
        for i in far_first(nz):
            push(CM.at[at_z(i)], CR.at[z], once_s.at[CMS], once_r.at[CMS], sp=at_z(i))
        CR[z] = CM[z]

    tiles = max(1, tok // 128)
    TR = tok // tiles

    def values_tile(i):
        rows = pl.ds(i * TR, TR)
        rounded = (L[rows, :].astype(f32) * scale[0:1] + shift[0:1]).astype(bf16)
        XM[rows, :] = rounded
        PVG[rows, :] = dot(rounded, VG[...]).astype(bf16)
        PLOW[rows, :] = dot(rounded, LOWT[...], NT).astype(bf16)

    def decays_tile(i):
        low = PLOW[pl.ds(i * TR, TR), :]
        for d, mask in ((0, low_b), (1, up_b)):
            steps = decays(low, d)
            for b in range(i * TR // BLOCK, (i + 1) * TR // BLOCK):
                at = b * BLOCK - i * TR
                ex = added[d][:, b * BLOCK : (b + 1) * BLOCK]
                cum = dot(mask.astype(f32), steps[at : at + BLOCK], precision=highest) + jnp.sum(
                    jnp.where(mask, ex, 0.0), axis=1, keepdims=True
                )
                total = cum[BLOCK - 1 : BLOCK] if d == 0 else cum[0:1]
                block_rows = slice(b * BLOCK, (b + 1) * BLOCK)
                EC[d, block_rows, :] = jnp.exp(cum)
                EI[d, block_rows, :] = jnp.exp(-cum)
                EO[d, block_rows, :] = jnp.exp(total - cum)
                TD[d, b] = total

    pieces = [f for i in range(tiles) for f in ((values_tile, i), (decays_tile, i))]
    for n, (piece, i) in enumerate(pieces):
        piece(i)
        if n < 3:
            first, last = 12 + n, (13 + n if n + 1 < min(3, len(pieces)) else nz - 1)

            @pl.when(core == 1)
            def _():
                w_take(first, last)
                if last == nz - 1:
                    context_states()

    @pl.when(core == 0)
    def _():
        all_in(WD, W.at[pl.ds(0, (nz - 1) * KR), :])
        context_states()

    sum_f, sum_b = jnp.zeros((1, DK), f32), jnp.zeros((1, DK), f32)
    for b in range(nb):
        OFF[0, b] = sum_f
        OFF[1, nb - 1 - b] = sum_b
        sum_f = sum_f + TD[0, b]
        sum_b = sum_b + TD[1, nb - 1 - b]
    DM[0] = sum_f
    DM[1] = sum_b
    for i in far_first(nz):
        push(DM.at[p], DR.at[p, z], once_s.at[DMS], once_r.at[DMS], sp=at_z(i))
    sent(CMS, CM.at[pl.ds(0, nz - 1)])
    sent(DMS, DR.at[0, pl.ds(0, nz - 1)])
    DR[p, z] = DM[p]

    QT = min(tok, 256)

    def project_qk(i, carry):
        rows = pl.ds(al(i * QT, QT), QT)
        PQK[rows, :] = dot(XM[rows, :], W[...]).astype(bf16)
        return carry

    lax.fori_loop(0, tok // QT, project_qk, 0)

    half = DK // 2
    for b in range(nb):
        rows = slice(b * BLOCK, (b + 1) * BLOCK)
        place = pl.ds(z * nb + b, 1)
        row_cos, row_sin = RT[0, place, :], RT[1, place, :]

        def rotated(values):
            first, second = values[:, :half], values[:, half:]
            return jnp.concatenate(
                [
                    first * row_cos + pltpu.roll(first, half // 2, 1) * row_sin,
                    second * CT[0] + pltpu.roll(second, half // 2, 1) * CT[1],
                ],
                axis=1,
            )

        q = rotated(PQK[rows, :DK].astype(f32)) * DK ** (-0.5)
        k = rotated(PQK[rows, DK:].astype(f32))
        v = PVG[rows, 0:VC]
        QK[rows, :DK] = q
        QK[rows, DK:] = k
        for d in range(2):
            U[d, b] = dot2(v, k * EO[d, rows, :], TN)

    fwd, bwd = jnp.zeros((VC, DK), f32), jnp.zeros((VC, DK), f32)
    for b in range(nb):
        e = nb - 1 - b
        PF[0, b] = fwd
        PF[1, e] = bwd
        fwd = jnp.exp(TD[0, b]) * fwd + U[0, b]
        bwd = jnp.exp(TD[1, e]) * bwd + U[1, e]
    LM[...] = message(fwd, bwd)
    for i in far_first(nz):
        push(LM.at[at_z(i)], LR.at[z], once_s.at[LMS], once_r.at[LMS], sp=at_z(i))
    sent(LMS, LM.at[pl.ds(0, nz - 1)])
    LR[z] = LM[z]

    for b in range(nb):
        rows = slice(b * BLOCK, (b + 1) * BLOCK)
        q, k = QK[rows, :DK], QK[rows, DK:]
        scores = jnp.zeros((BLOCK, BLOCK), f32)
        total = jnp.zeros((BLOCK, VC), f32)
        for d, mask in ((0, low_b), (1, up_b)):
            q_in = q * EC[d, rows, :]
            scores = scores + jnp.where(mask, dot3(q_in, k * EI[d, rows, :], NT), 0.0)
            total = total + dot3(q_in, PF[d, b], NT)
            high, low = halves(q_in * jnp.exp(OFF[d, b]))
            QD[0, rows, d * DK : (d + 1) * DK] = high
            QD[1, rows, d * DK : (d + 1) * DK] = low
        high, low = halves(scores)
        v = PVG[rows, 0:VC]
        O[rows, :] = total + (dot(high, v) + dot(low, v))

    all_in(CMS, CR.at[pl.ds(0, nz - 1)])
    all_in(DMS, DR.at[0, pl.ds(0, nz - 1)])
    for i in range(1, share):
        push(
            DR.at[p],
            DR.at[p],
            once_s.at[DXS],
            once_r.at[DXS],
            tp=h * share + lax.rem(p + i, share),
        )
    sent(DXS, DR.at[pl.ds(0, share - 1)])
    all_in(LMS, LR.at[pl.ds(0, nz - 1)])
    all_in(DXS, DR.at[pl.ds(0, share - 1)])

    def context_chain(s, carry):
        fwd, bwd = carry
        e = nz - 1 - s
        fwd = jnp.exp(DR[2, s]) * fwd + CR[s].astype(f32)[:dvs]
        bwd = jnp.exp(DR[3, e]) * bwd + CR[e].astype(f32)[dvs:]
        return fwd, bwd

    slice0 = jnp.zeros((dvs, DK), f32)
    fwd, bwd = lax.fori_loop(0, nz, context_chain, (slice0, slice0))
    fwd_in, bwd_in = [], [None] * nz
    for s in range(nz):
        e = nz - 1 - s
        fwd_in.append(fwd)
        bwd_in[e] = bwd
        fwd = jnp.exp(DR[0, s]) * fwd + LR[s].astype(f32)[:dvs]
        bwd = jnp.exp(DR[1, e]) * bwd + LR[e].astype(f32)[dvs:]
    for s in range(nz):
        RO[s] = jnp.concatenate([fwd_in[s], bwd_in[s]], axis=0)
    for i in far_first(nz):
        push(RO.at[at_z(i)], RR.at[z], once_s.at[ROS], once_r.at[ROS], sp=at_z(i))
    sent(ROS, RO.at[pl.ds(0, nz - 1)])
    RR[z] = RO[z]
    gate_rows = silu(PVG[:, VC:].astype(f32)) * gain[:, pl.ds(al(p * VC, VC), VC)]
    all_in(ROS, RR.at[pl.ds(0, nz - 1)])
    back = RR[...]
    start, start_low = halves(
        jnp.concatenate([back[:, :dvs].reshape(VC, DK), back[:, dvs:].reshape(VC, DK)], axis=1)
    )
    mixture = O[...] + (
        dot(QD[0], start, NT) + (dot(QD[0], start_low, NT) + dot(QD[1], start, NT))
    )

    SS[p] = dot(jnp.ones((8, VC), f32), mixture * mixture, NT, precision=highest)
    for i in range(1, share):
        push(
            SS.at[p],
            SS.at[p],
            once_s.at[SSS],
            once_r.at[SSS],
            tp=h * share + lax.rem(p + i, share),
        )
    sent(SSS, SS.at[pl.ds(0, share - 1)])
    GT[...] = (mixture * gate_rows).reshape(nt, TB, VC)

    def owner(q, j):
        chip = jnp.where(q // 2 == 0, 2 * h - j + nx, 2 * h + 1 + j)
        return lax.rem(chip, nx) * 2 + q % 2

    lanes = pl.ds(al(p * VC, VC), VC)
    for i in range(1, share):
        q = lax.rem(p + i, share)
        for j in range(heads):
            push(
                GT.at[owner(q, j)],
                GR.at[j, :, lanes],
                once_s.at[GRS],
                once_r.at[GRS],
                tp=h * share + q,
            )
    sent(GRS, GT.at[pl.ds(0, (share - 1) * heads)])
    for j in range(heads):
        GR[j, :, lanes] = GT[owner(p, j)]
    all_in(SSS, SS.at[pl.ds(0, share - 1)])
    squares = SS[0]
    for i in range(1, share):
        squares = squares + SS[i]
    IV[...] = lax.rsqrt(squares / (share * VC) + norm_eps).T.reshape(nt, TB, 8)
    all_in(WOUT, WO.at[pl.ds(0, (share - 1) * VC), :])
    all_in(GRS, GT.at[pl.ds(0, (share - 1) * heads)])

    left = jnp.concatenate(
        [(GR[j] * IV[owner(p, j)][:, 0:1]).astype(bf16) for j in range(heads)], axis=0
    )
    NC = D // 4
    for n in range(4):
        partial = dot(left, WO[:, n * NC : (n + 1) * NC]).reshape(heads, TB, NC)
        ACC[:, n * NC : (n + 1) * NC] = partial[0]
        PS[:, n] = partial.astype(bf16)
        for j in range(heads - 1, 0, -1):
            push(PS.at[j, n], PR.at[j, n], once_s.at[PRS], once_r.at[PRS], tp=owner(p, j))
    branch = ACC[...]
    if heads > 1:
        sent(PRS, PS.at[pl.ds(0, heads - 1)])
        all_in(PRS, PR.at[pl.ds(0, heads - 1)])
    for j in range(1, heads):
        branch = branch + jnp.concatenate([PR[j, n].astype(f32) for n in range(4)], axis=1)
    own = L[pl.ds(al(t * TB, TB), TB), :].astype(f32)
    gates = M[0:1, 2 * D :] + mod_b[:, 2 * D :]
    summed = residual_scale * own + gates * branch
    centered = summed - jnp.mean(summed, axis=1, keepdims=True)
    variance = jnp.mean(centered * centered, axis=1, keepdims=True)
    out[...] = (
        centered * lax.rsqrt(variance + norm_eps) * final_g[...] + final_b[...]
    ).astype(out.dtype)
    for copy in pending:
        copy.wait_send()

    @pl.when(core == 0)
    def _():
        waiter(L.at[pl.ds(0, 2 * (nx - 1) * TB), :], once_s.at[LX], once_r.at[LX]).wait_send()
        waiter(L.at[rest, :], once_s.at[LD], once_r.at[LD]).wait_send()

    @pl.when(core == 1)
    def _():
        view = W.at[pl.ds(0, (nz - 1) * KR), :]
        waiter(view, once_s.at[WZ], once_r.at[WZ]).wait_send()
        waiter(view, once_s.at[WD], once_r.at[WD]).wait_send()
        waiter(L.at[pl.ds(0, TB), :], once_s.at[LD], once_r.at[LD]).wait_send()


def body(
    nz,
    nt,
    latent,
    context,
    condition,
    context_condition,
    mod_weight,
    mod_bias,
    query_weight,
    key_weight,
    value_weight,
    out_gate_weight,
    decay_in_weight,
    decay_weight,
    decay_bias,
    extra_decay,
    norm_gain,
    out_weight,
    final_gain,
    final_bias,
):
    heads = ATTENTION_HEADS
    share = nt // heads
    D = latent.shape[1]
    TB = latent.shape[0]
    tok = TB * nt
    DK = query_weight.shape[1] // heads
    VC = value_weight.shape[1]
    MC = mod_weight.shape[1]
    nb = tok // BLOCK
    row_tab, col_tab = rotary_tables(nz * nb, DK // 2)
    dvs = VC // nz
    vmem = pl.BlockSpec(memory_space=pltpu.VMEM)
    hbm = pl.BlockSpec(memory_space=pl.ANY)
    dma = pltpu.SemaphoreType.DMA
    scratch = [
        pltpu.VMEM((tok, D), bf16),
        pltpu.VMEM((tok, D), bf16),
        pltpu.VMEM((D, 2 * DK), bf16),
        pltpu.VMEM((D, 2 * VC), bf16),
        pltpu.VMEM((share * VC, D), bf16),
        pltpu.VMEM((2, 3 * D), f32),
        pltpu.VMEM((nz, 2, MC), f32),
        pltpu.VMEM((tok, 2 * VC), bf16),
        pltpu.VMEM((tok, decay_in_weight.shape[1]), bf16),
        pltpu.VMEM((tok, 2 * DK), bf16),
        pltpu.VMEM((tok, 2 * DK), f32),
        pltpu.VMEM((2, tok, 2 * DK), bf16),
        pltpu.VMEM((tok, VC), f32),
        pltpu.VMEM((2, nb, VC, DK), f32),
        pltpu.VMEM((2, nb, 1, DK), f32),
        pltpu.VMEM((2, nb, VC, DK), f32),
        pltpu.VMEM((2, nb, 1, DK), f32),
        pltpu.VMEM((nz, 2 * dvs, DK), bf16),
        pltpu.VMEM((nz, 2 * dvs, DK), bf16),
        pltpu.VMEM((nz, 2 * dvs, DK), bf16),
        pltpu.VMEM((nz, 2 * dvs, DK), bf16),
        pltpu.VMEM((share, 1, DK), f32),
        pltpu.VMEM((share, nz, 1, DK), f32),
        pltpu.VMEM((nz, 2 * dvs, DK), f32),
        pltpu.VMEM((nz, 2 * dvs, DK), f32),
        pltpu.VMEM((share, 8, tok), f32),
        pltpu.VMEM((nt, TB, VC), f32),
        pltpu.VMEM((heads, TB, share * VC), f32),
        pltpu.VMEM((TB, D), f32),
        pltpu.VMEM((heads, 4, TB, D // 4), bf16),
        pltpu.VMEM((heads, 4, TB, D // 4), bf16),
        pltpu.VMEM((nt, TB, 8), f32),
        *[
            pltpu.VMEM(shape, kind)
            for shape, kind in (
                ((1, condition.shape[0]), f32),
                ((1, context_condition.shape[0]), f32),
                (mod_weight.shape, bf16),
                ((1, mod_bias.shape[0]), f32),
                (decay_weight.shape, bf16),
                (decay_bias.shape, f32),
                (extra_decay.shape, f32),
                ((1, norm_gain.shape[0]), f32),
                ((1, D), f32),
                ((1, D), f32),
            )
        ],
        pltpu.VMEM(context.shape, bf16),
        pltpu.VMEM((decay_in_weight.shape[1], D), bf16),
        pltpu.VMEM(row_tab.shape, f32),
        pltpu.VMEM(col_tab.shape, f32),
        pltpu.VMEM((2, tok, DK), f32),
        pltpu.VMEM((2, tok, DK), f32),
        pltpu.VMEM((2, tok, DK), f32),
        dma((20,)),
        dma((15,)),
        dma((15,)),
        dma((4 * nz,)),
        dma((2 * nt,)),
    ]
    in_specs = [hbm] * 20
    return pl.pallas_call(
        functools.partial(kernel, nz, nt, heads),
        out_shape=pltpu.VMEM((TB, D), bf16),
        in_specs=in_specs,
        out_specs=vmem,
        scratch_shapes=scratch,
        compiler_params=pltpu.CompilerParams(
            collective_id=0, has_side_effects=True, vmem_limit_bytes=58 * 1024 * 1024
        ),
        name="layer",
    )(
        latent,
        context,
        condition.reshape(1, -1),
        context_condition.reshape(1, -1),
        mod_weight,
        mod_bias.reshape(1, -1),
        query_weight,
        key_weight,
        value_weight,
        out_gate_weight,
        decay_in_weight.T,
        decay_weight,
        decay_bias,
        extra_decay,
        norm_gain.reshape(1, -1),
        out_weight,
        final_gain.reshape(1, -1),
        final_bias.reshape(1, -1),
        jnp.asarray(row_tab),
        jnp.asarray(col_tab),
    )


def solution(mesh):
    placed = (
        P(("grp", "sp", "tp"), None),
        P(("grp", "sp"), None),
        P(("grp", "sp")),
        P("sp"),
        P("sp", "tp"),
        P(),
        P("sp", None),
        P("sp", None),
        P(None, "tp"),
        P(None, "tp"),
        P(),
        P(),
        P(),
        P(None, None, "sp"),
        P(),
        P("tp", None),
        P(),
        P(),
    )
    return jax.shard_map(
        functools.partial(body, mesh.shape["sp"], mesh.shape["tp"]),
        mesh=mesh,
        in_specs=placed,
        out_specs=P(("grp", "sp", "tp"), None),
        check_vma=False,
    )
```

```python
import functools

import numpy as np
import jax
import jax.numpy as jnp
from jax import lax
from jax.experimental import pallas as pl
from jax.experimental.pallas import tpu as pltpu
from jax.sharding import PartitionSpec as P

ATTENTION_HEADS = 4
DV = 512
BLOCK = 64
GRID_W = 64

norm_eps = 1e-05
gate_scale = 16.0
rope_base = 10000.0
residual_scale = 2.0**0.5
highest = lax.Precision.HIGHEST
f32 = jnp.float32
bf16 = jnp.bfloat16

NT = (((1,), (1,)), ((), ()))
TN = (((0,), (0,)), ((), ()))


def dot(a, b, dims=None, precision=None):
    if dims is None:
        dims = (((1,), (0,)), ((), ()))
    return lax.dot_general(a, b, dims, precision=precision, preferred_element_type=f32)


def halves(a):
    high = a.astype(bf16)
    return high, (a - high.astype(f32)).astype(bf16)


def dot2(a, b, dims=None):
    high, low = halves(b)
    return dot(a, high, dims) + dot(a, low, dims)


def dot3(a, b, dims=None):
    a_high, a_low = halves(a)
    b_high, b_low = halves(b)
    return dot(a_high, b_high, dims) + (dot(a_high, b_low, dims) + dot(a_low, b_high, dims))


def log_sigmoid(v):
    return jnp.minimum(v, 0.0) - jnp.log1p(jnp.exp(-jnp.abs(v)))


def silu(v):
    return v / (1.0 + jnp.exp(-v))


def rotary_tables(rows, half):
    quarter = half // 2
    frequency = (rope_base ** (-np.arange(quarter, dtype=np.float64) / quarter)).astype(np.float32)

    def table(places):
        angle = (np.arange(places, dtype=np.float32)[:, None] * frequency).astype(np.float64)
        cosine = np.cos(angle)
        sine = np.sin(angle)
        return np.stack(
            [np.concatenate([cosine, cosine], 1), np.concatenate([-sine, sine], 1)]
        ).astype(np.float32)

    return table(rows), table(GRID_W)


def spread(n, j):
    long, short = n // 2, (n - 1) // 2
    right, left = (long, short) if j % 2 == 0 else (short, long)
    steps = {a: [a + 1] for a in range(1, right)} | {-a: [-a - 1] for a in range(1, left)}
    steps[0] = ([1] if right else []) + ([-1] if left else [])
    due = [o for a in range(1, long + 1) for o in (a, -a) if o <= right and o >= -left]
    return due, steps


def kernel(
    nz,
    nt,
    heads,
    lat_in,
    ctx_hbm,
    cond_hbm,
    ctx_cond_hbm,
    mod_w_hbm,
    mod_b_hbm,
    qw,
    kw,
    vw,
    gw,
    low_hbm,
    decay_w_hbm,
    decay_b_hbm,
    extra_hbm,
    gain_hbm,
    out_w,
    final_g_hbm,
    final_b_hbm,
    row_hbm,
    col_hbm,
    out,
    L,
    XM,
    W,
    VG,
    WO,
    M,
    mod_part,
    PVG,
    PLOW,
    PQK,
    QK,
    QD,
    O,
    U,
    TD,
    PF,
    OFF,
    LM,
    LR,
    CM,
    CR,
    DM,
    DR,
    RO,
    RR,
    SS,
    GT,
    GR,
    ACC,
    PS,
    PR,
    IV,
    cond,
    ctx_cond,
    mod_w,
    mod_b,
    decay_w,
    decay_b,
    extra,
    gain,
    final_g,
    final_b,
    CX,
    LOWT,
    RT,
    CT,
    EC,
    EI,
    EO,
    loc_sem,
    once_s,
    once_r,
    wz_r,
    lx_r,
):
    z = lax.axis_index("sp")
    t = lax.axis_index("tp")
    share = nt // heads
    h = t // share
    p = t % share
    core = t % 2
    x = t // 2
    nx = nt // 2
    partner = t + 1 - 2 * core
    D = lat_in.shape[1]
    TB = lat_in.shape[0]
    tok = TB * nt
    KR = qw.shape[0]
    DK = qw.shape[1] // heads
    HC = DK // 2
    VC = vw.shape[1]
    MC = mod_w_hbm.shape[1]
    nb = tok // BLOCK
    dvs = VC // nz
    pending = []
    MP, MG, WZ, WD, LX, LD, WOUT, LMS, CMS, DMS, ROS, SSS, GRS, PRS, DXS = range(15)

    def push(src, dst, ssem, rsem, **where):
        pltpu.make_async_remote_copy(
            src_ref=src,
            dst_ref=dst,
            send_sem=ssem,
            recv_sem=rsem,
            device_id=where,
            device_id_type=pl.DeviceIdType.MESH,
        ).start()

    def waiter(view, ssem, rsem):
        return pltpu.make_async_remote_copy(
            src_ref=view,
            dst_ref=view,
            send_sem=ssem,
            recv_sem=rsem,
            device_id={"tp": partner},
            device_id_type=pl.DeviceIdType.MESH,
        )

    def all_in(kind, view):
        waiter(view, once_s.at[kind], once_r.at[kind]).wait_recv()

    def sent(kind, view):
        pending.append(waiter(view, once_s.at[kind], once_r.at[kind]))

    def far_first(n):
        return sorted(range(1, n), key=lambda i: (-min(i, n - i), i))

    def at_z(i):
        return lax.rem(z + i + nz, nz)

    def at_t(i):
        return lax.rem(t + i + nt, nt)

    def at_x(i):
        return lax.rem(x + i + nx, nx)

    def al(v, m):
        return pl.multiple_of(v, m)

    def w_at(zz, j, parts=2):
        rows = KR // parts
        first = zz * KR + (j % parts) * rows
        return W.at[pl.ds(al(first, rows), rows), pl.ds((j // parts) * DK, DK)]

    def l_at(xx, j):
        rows = pl.ds(al((xx * 2 + j // 2) * TB, TB), TB)
        return L.at[rows, pl.ds((j % 2) * (D // 2), D // 2)]

    head_cols = pl.ds(al(h * DK, DK), DK)
    loads = [
        (cond_hbm, cond),
        (ctx_cond_hbm, ctx_cond),
        (mod_w_hbm, mod_w),
        (lat_in, L.at[pl.ds(al(t * TB, TB), TB), :]),
        (qw.at[:, head_cols], w_at(z, 0, 1)),
        (kw.at[:, head_cols], w_at(z, 1, 1)),
        (out_w, WO.at[pl.ds(al(p * VC, VC), VC), :]),
        (vw, VG.at[:, pl.ds(0, VC)]),
        (gw, VG.at[:, pl.ds(VC, VC)]),
        (ctx_hbm, CX),
        (low_hbm, LOWT),
        (mod_b_hbm, mod_b),
        (decay_w_hbm, decay_w),
        (decay_b_hbm, decay_b),
        (extra_hbm, extra),
        (gain_hbm, gain),
        (final_g_hbm, final_g),
        (final_b_hbm, final_b),
        (row_hbm, RT),
        (col_hbm, CT),
    ]
    local = [
        pltpu.make_async_copy(src, dst, loc_sem.at[i]) for i, (src, dst) in enumerate(loads)
    ]
    barrier = pltpu.get_barrier_semaphore()
    for i in far_first(nz):
        pl.semaphore_signal(
            barrier, inc=1, device_id={"sp": at_z(i)}, device_id_type=pl.DeviceIdType.MESH
        )
    for i in far_first(nt):
        pl.semaphore_signal(
            barrier, inc=1, device_id={"tp": at_t(i)}, device_id_type=pl.DeviceIdType.MESH
        )
    for copy in local[:6]:
        copy.start()
    for copy in local[:3]:
        copy.wait()

    both = jnp.concatenate([cond[...], ctx_cond[...], jnp.zeros((6, cond.shape[1]), f32)], axis=0)
    part = dot(silu(both).astype(bf16), mod_w[...])
    mod_part[z] = part[0:2]

    for copy in local[3:6]:
        copy.wait()
    pl.semaphore_wait(barrier, nz - 1 + nt - 1)

    for i in far_first(nz):
        push(mod_part.at[z], mod_part.at[z], once_s.at[MP], once_r.at[MP], sp=at_z(i))
    sent(MP, mod_part.at[pl.ds(0, nz - 1)])

    def ring(n, chunks, at, region, whole, far, sem_r, kind, share_kind):
        plans = [spread(n, j) for j in range(chunks)]

        def hand_on(o, j):
            src = region(at(-o), j)
            for c in plans[j][1].get(o, []):
                sem = sem_r.at[(c % n) * chunks + j]
                push(src, src, once_s.at[kind], sem, **far(c - o))

        def take(first, last):
            for i in range(first, min(last, n - 1)):
                for j in range(chunks):
                    o = plans[j][0][i]
                    sem = sem_r.at[(o % n) * chunks + j]
                    waiter(region(at(-o), j), once_s.at[kind], sem).wait_recv()
                    hand_on(o, j)
                src = whole(at(-plans[0][0][i]))
                push(src, src, once_s.at[share_kind], once_r.at[share_kind], tp=partner)

        return hand_on, take

    def l_whole(xx):
        return L.at[pl.ds(al(xx * 2 * TB, 2 * TB), 2 * TB), :]

    def w_whole(zz):
        return W.at[pl.ds(al(zz * KR, KR), KR), :]

    l_on, l_take = ring(
        nx, 4, at_x, l_at, l_whole, lambda i: {"tp": at_x(i) * 2 + core}, lx_r, LX, LD
    )
    w_on, w_take = ring(nz, 4, at_z, w_at, w_whole, lambda i: {"sp": at_z(i)}, wz_r, WZ, WD)
    own_rows = L.at[pl.ds(al(t * TB, TB), TB), :]
    rest = pl.ds(0, (2 * nx - 1) * TB)

    def load_rest():
        for copy in local[6:]:
            copy.start()

    @pl.when(core == 0)
    def _():
        for j in range(2):
            l_on(0, j)
        push(own_rows, own_rows, once_s.at[LD], once_r.at[LD], tp=partner)
        all_in(LD, L.at[pl.ds(0, TB), :])
        for j in range(2, 4):
            l_on(0, j)
        load_rest()
        l_take(0, 4)

    @pl.when(core == 1)
    def _():
        push(own_rows, own_rows, once_s.at[LD], once_r.at[LD], tp=partner)
        for j in range(4):
            w_on(0, j)
        load_rest()
        w_take(0, 6)

    def modulation_sums():
        all_in(MP, mod_part.at[pl.ds(0, nz - 1)])
        sums = mod_part[0]
        for i in range(1, nz):
            sums = sums + mod_part[i]
        cols = pl.ds(al(t * MC, 128), MC)
        M[:, cols] = sums
        for i in far_first(nt):
            push(M.at[:, cols], M.at[:, cols], once_s.at[MG], once_r.at[MG], tp=at_t(i))
        sent(MG, M.at[:, pl.ds(0, (nt - 1) * MC)])

    modulation_sums()

    @pl.when(core == 0)
    def _():
        l_take(4, nx - 1)

    @pl.when(core == 1)
    def _():
        w_take(6, 12)

    local[6].wait()
    proj_rows = WO.at[pl.ds(al(p * VC, VC), VC), :]
    for i in range(1, share):
        push(
            proj_rows,
            proj_rows,
            once_s.at[WOUT],
            once_r.at[WOUT],
            tp=h * share + lax.rem(p + i, share),
        )
    sent(WOUT, WO.at[pl.ds(0, (share - 1) * VC), :])
    all_in(MG, M.at[:, pl.ds(0, (nt - 1) * MC)])
    for copy in local[7:]:
        copy.wait()

    mod = M[...] + mod_b[...]
    shift, scale = mod[:, :D], 1.0 + mod[:, D : 2 * D]
    bias = decay_b[:, pl.ds(al(h * DK, DK), DK)]
    rank = decay_w.shape[1]
    zero = jnp.zeros((rank, DK), bf16)
    maps = [
        jnp.concatenate([decay_w[0, :, head_cols], zero], axis=0),
        jnp.concatenate([zero, decay_w[1, :, head_cols]], axis=0),
    ]

    def triangles(size):
        row = lax.broadcasted_iota(jnp.int32, (size, size), 0)
        col = lax.broadcasted_iota(jnp.int32, (size, size), 1)
        return row >= col, row <= col

    low_b, up_b = triangles(BLOCK)
    added = [extra[d, pl.ds(h, 1), :] for d in range(2)]

    def decays(low, d):
        return log_sigmoid(dot(low, maps[d]) + bias[d : d + 1]) * (1.0 / gate_scale)

    @pl.when(core == 1)
    def _():
        all_in(LD, L.at[rest, :])

    def message(forward, backward):
        return jnp.concatenate(
            [forward.reshape(nz, dvs, DK), backward.reshape(nz, dvs, DK)], axis=1
        ).astype(bf16)

    def context_states():
        ctx_rows = (CX[...].astype(f32) * scale[1:2] + shift[1:2]).astype(bf16)
        ctx_values = dot(ctx_rows, VG[:, 0:VC]).astype(bf16)
        ctx_low = dot(ctx_rows, LOWT[...], NT).astype(bf16)
        CB = ctx_hbm.shape[0]
        low_c, up_c = triangles(CB)
        cum_f = dot(low_c.astype(f32), decays(ctx_low, 0), precision=highest)
        cum_b = dot(up_c.astype(f32), decays(ctx_low, 1), precision=highest)
        tot_cf, tot_cb = cum_f[CB - 1 : CB], cum_b[0:1]
        DM[1, 0:1, :] = tot_cf
        DM[1, 1:2, :] = tot_cb
        ctx_keys = dot(ctx_rows, W[:, DK : 2 * DK]).astype(bf16).astype(f32)
        CM[...] = message(
            dot2(ctx_values, ctx_keys * jnp.exp(tot_cf - cum_f), TN),
            dot2(ctx_values, ctx_keys * jnp.exp(tot_cb - cum_b), TN),
        )
        for i in far_first(nz):
            push(CM.at[at_z(i)], CR.at[z], once_s.at[CMS], once_r.at[CMS], sp=at_z(i))
        CR[z] = CM[z]

    tiles = max(1, tok // 128)
    TR = tok // tiles

    def values_tile(i):
        rows = pl.ds(i * TR, TR)
        rounded = (L[rows, :].astype(f32) * scale[0:1] + shift[0:1]).astype(bf16)
        XM[rows, :] = rounded
        PVG[rows, :] = dot(rounded, VG[...]).astype(bf16)
        PLOW[rows, :] = dot(rounded, LOWT[...], NT).astype(bf16)

    def decays_tile(i):
        low = PLOW[pl.ds(i * TR, TR), :]
        for d, mask in ((0, low_b), (1, up_b)):
            steps = decays(low, d)
            for b in range(i * TR // BLOCK, (i + 1) * TR // BLOCK):
                at = b * BLOCK - i * TR
                ex = added[d][:, b * BLOCK : (b + 1) * BLOCK]
                cum = dot(mask.astype(f32), steps[at : at + BLOCK], precision=highest) + jnp.sum(
                    jnp.where(mask, ex, 0.0), axis=1, keepdims=True
                )
                total = cum[BLOCK - 1 : BLOCK] if d == 0 else cum[0:1]
                block_rows = slice(b * BLOCK, (b + 1) * BLOCK)
                EC[d, block_rows, :] = jnp.exp(cum)
                EI[d, block_rows, :] = jnp.exp(-cum)
                EO[d, block_rows, :] = jnp.exp(total - cum)
                TD[d, b] = total

    pieces = [f for i in range(tiles) for f in ((values_tile, i), (decays_tile, i))]
    for n, (piece, i) in enumerate(pieces):
        piece(i)
        if n < 3:
            first, last = 12 + n, (13 + n if n + 1 < min(3, len(pieces)) else nz - 1)

            @pl.when(core == 1)
            def _():
                w_take(first, last)
                if last == nz - 1:
                    context_states()

    @pl.when(core == 0)
    def _():
        all_in(WD, W.at[pl.ds(0, (nz - 1) * KR), :])
        context_states()

    sum_f, sum_b = jnp.zeros((1, DK), f32), jnp.zeros((1, DK), f32)
    for b in range(nb):
        OFF[0, b] = sum_f
        OFF[1, nb - 1 - b] = sum_b
        sum_f = sum_f + TD[0, b]
        sum_b = sum_b + TD[1, nb - 1 - b]
    DM[0, 0:1, :] = sum_f
    DM[0, 1:2, :] = sum_b
    for i in far_first(nz):
        push(DM.at[core], DR.at[core, z], once_s.at[DMS], once_r.at[DMS], sp=at_z(i))
    sent(CMS, CM.at[pl.ds(0, nz - 1)])
    sent(DMS, DR.at[0, pl.ds(0, nz - 1)])
    DR[core, z] = DM[core]

    QT = min(tok, 256)

    def project_qk(i, carry):
        rows = pl.ds(al(i * QT, QT), QT)
        PQK[rows, :] = dot(XM[rows, :], W[...]).astype(bf16)
        return carry

    lax.fori_loop(0, tok // QT, project_qk, 0)

    half = DK // 2
    for b in range(nb):
        rows = slice(b * BLOCK, (b + 1) * BLOCK)
        place = pl.ds(z * nb + b, 1)
        row_cos, row_sin = RT[0, place, :], RT[1, place, :]

        def rotated(values):
            first, second = values[:, :half], values[:, half:]
            return jnp.concatenate(
                [
                    first * row_cos + pltpu.roll(first, half // 2, 1) * row_sin,
                    second * CT[0] + pltpu.roll(second, half // 2, 1) * CT[1],
                ],
                axis=1,
            )

        q = rotated(PQK[rows, :DK].astype(f32)) * DK ** (-0.5)
        k = rotated(PQK[rows, DK:].astype(f32))
        v = PVG[rows, 0:VC]
        QK[rows, :DK] = q
        QK[rows, DK:] = k
        for d in range(2):
            U[d, b] = dot2(v, k * EO[d, rows, :], TN)

    fwd, bwd = jnp.zeros((VC, DK), f32), jnp.zeros((VC, DK), f32)
    for b in range(nb):
        e = nb - 1 - b
        PF[0, b] = fwd
        PF[1, e] = bwd
        fwd = jnp.exp(TD[0, b]) * fwd + U[0, b]
        bwd = jnp.exp(TD[1, e]) * bwd + U[1, e]
    LM[...] = message(fwd, bwd)
    for i in far_first(nz):
        push(LM.at[at_z(i)], LR.at[z], once_s.at[LMS], once_r.at[LMS], sp=at_z(i))
    sent(LMS, LM.at[pl.ds(0, nz - 1)])
    LR[z] = LM[z]

    for b in range(nb):
        rows = slice(b * BLOCK, (b + 1) * BLOCK)
        q, k = QK[rows, :DK], QK[rows, DK:]
        scores = jnp.zeros((BLOCK, BLOCK), f32)
        total = jnp.zeros((BLOCK, VC), f32)
        for d, mask in ((0, low_b), (1, up_b)):
            q_in = q * EC[d, rows, :]
            scores = scores + jnp.where(mask, dot3(q_in, k * EI[d, rows, :], NT), 0.0)
            total = total + dot3(q_in, PF[d, b], NT)
            high, low = halves(q_in * jnp.exp(OFF[d, b]))
            QD[0, rows, d * DK : (d + 1) * DK] = high
            QD[1, rows, d * DK : (d + 1) * DK] = low
        high, low = halves(scores)
        v = PVG[rows, 0:VC]
        O[rows, :] = total + (dot(high, v) + dot(low, v))

    all_in(CMS, CR.at[pl.ds(0, nz - 1)])
    all_in(DMS, DR.at[0, pl.ds(0, nz - 1)])
    push(DR.at[core], DR.at[core], once_s.at[DXS], once_r.at[DXS], tp=partner)
    sent(DXS, DR.at[0])
    all_in(LMS, LR.at[pl.ds(0, nz - 1)])
    all_in(DXS, DR.at[0])

    def context_chain(s, carry):
        fwd, bwd = carry
        e = nz - 1 - s
        fwd = jnp.exp(DR[1, s, 0:1]) * fwd + CR[s].astype(f32)[:dvs]
        bwd = jnp.exp(DR[1, e, 1:2]) * bwd + CR[e].astype(f32)[dvs:]
        return fwd, bwd

    slice0 = jnp.zeros((dvs, DK), f32)
    fwd, bwd = lax.fori_loop(0, nz, context_chain, (slice0, slice0))
    fwd_in, bwd_in = [], [None] * nz
    for s in range(nz):
        e = nz - 1 - s
        fwd_in.append(fwd)
        bwd_in[e] = bwd
        fwd = jnp.exp(DR[0, s, 0:1]) * fwd + LR[s].astype(f32)[:dvs]
        bwd = jnp.exp(DR[0, e, 1:2]) * bwd + LR[e].astype(f32)[dvs:]
    for s in range(nz):
        RO[s] = jnp.concatenate([fwd_in[s], bwd_in[s]], axis=0).astype(bf16)
    for i in far_first(nz):
        push(RO.at[at_z(i)], RR.at[z], once_s.at[ROS], once_r.at[ROS], sp=at_z(i))
    sent(ROS, RO.at[pl.ds(0, nz - 1)])
    RR[z] = RO[z]
    gate_rows = silu(PVG[:, VC:].astype(f32)) * gain[:, pl.ds(al(p * VC, VC), VC)]
    all_in(ROS, RR.at[pl.ds(0, nz - 1)])
    back = RR[...].astype(f32)
    start = jnp.concatenate(
        [back[:, :dvs].reshape(VC, DK), back[:, dvs:].reshape(VC, DK)], axis=1
    ).astype(bf16)
    mixture = O[...] + (dot(QD[0], start, NT) + dot(QD[1], start, NT))

    SS[p] = dot(jnp.ones((8, VC), f32), mixture * mixture, NT, precision=highest)
    for i in range(1, share):
        push(
            SS.at[p],
            SS.at[p],
            once_s.at[SSS],
            once_r.at[SSS],
            tp=h * share + lax.rem(p + i, share),
        )
    sent(SSS, SS.at[pl.ds(0, share - 1)])
    GT[...] = (mixture * gate_rows).reshape(nt, TB, VC)

    def owner(q, j):
        chip = jnp.where(q // 2 == 0, 2 * h - j + nx, 2 * h + 1 + j)
        return lax.rem(chip, nx) * 2 + q % 2

    lanes = pl.ds(al(p * VC, VC), VC)
    for i in range(1, share):
        q = lax.rem(p + i, share)
        for j in range(heads):
            push(
                GT.at[owner(q, j)],
                GR.at[j, :, lanes],
                once_s.at[GRS],
                once_r.at[GRS],
                tp=h * share + q,
            )
    sent(GRS, GT.at[pl.ds(0, (share - 1) * heads)])
    for j in range(heads):
        GR[j, :, lanes] = GT[owner(p, j)]
    all_in(SSS, SS.at[pl.ds(0, share - 1)])
    squares = SS[0]
    for i in range(1, share):
        squares = squares + SS[i]
    IV[...] = lax.rsqrt(squares / (share * VC) + norm_eps).T.reshape(nt, TB, 8)
    all_in(WOUT, WO.at[pl.ds(0, (share - 1) * VC), :])
    all_in(GRS, GT.at[pl.ds(0, (share - 1) * heads)])

    left = jnp.concatenate(
        [(GR[j] * IV[owner(p, j)][:, 0:1]).astype(bf16) for j in range(heads)], axis=0
    )
    NC = D // 4
    for n in range(4):
        partial = dot(left, WO[:, n * NC : (n + 1) * NC]).reshape(heads, TB, NC)
        ACC[:, n * NC : (n + 1) * NC] = partial[0]
        PS[:, n] = partial.astype(bf16)
        for j in range(heads - 1, 0, -1):
            push(PS.at[j, n], PR.at[j, n], once_s.at[PRS], once_r.at[PRS], tp=owner(p, j))
    branch = ACC[...]
    if heads > 1:
        sent(PRS, PS.at[pl.ds(0, heads - 1)])
        all_in(PRS, PR.at[pl.ds(0, heads - 1)])
    for j in range(1, heads):
        branch = branch + jnp.concatenate([PR[j, n].astype(f32) for n in range(4)], axis=1)
    own = L[pl.ds(al(t * TB, TB), TB), :].astype(f32)
    gates = M[0:1, 2 * D :] + mod_b[:, 2 * D :]
    summed = residual_scale * own + gates * branch
    centered = summed - jnp.mean(summed, axis=1, keepdims=True)
    variance = jnp.mean(centered * centered, axis=1, keepdims=True)
    out[...] = (
        centered * lax.rsqrt(variance + norm_eps) * final_g[...] + final_b[...]
    ).astype(out.dtype)
    for copy in pending:
        copy.wait_send()

    @pl.when(core == 0)
    def _():
        waiter(L.at[pl.ds(0, 2 * (nx - 1) * TB), :], once_s.at[LX], once_r.at[LX]).wait_send()
        waiter(L.at[rest, :], once_s.at[LD], once_r.at[LD]).wait_send()

    @pl.when(core == 1)
    def _():
        view = W.at[pl.ds(0, (nz - 1) * KR), :]
        waiter(view, once_s.at[WZ], once_r.at[WZ]).wait_send()
        waiter(view, once_s.at[WD], once_r.at[WD]).wait_send()
        waiter(L.at[pl.ds(0, TB), :], once_s.at[LD], once_r.at[LD]).wait_send()


def body(
    nz,
    nt,
    latent,
    context,
    condition,
    context_condition,
    mod_weight,
    mod_bias,
    query_weight,
    key_weight,
    value_weight,
    out_gate_weight,
    decay_in_weight,
    decay_weight,
    decay_bias,
    extra_decay,
    norm_gain,
    out_weight,
    final_gain,
    final_bias,
):
    heads = ATTENTION_HEADS
    share = nt // heads
    D = latent.shape[1]
    TB = latent.shape[0]
    tok = TB * nt
    DK = query_weight.shape[1] // heads
    VC = value_weight.shape[1]
    MC = mod_weight.shape[1]
    nb = tok // BLOCK
    row_tab, col_tab = rotary_tables(nz * nb, DK // 2)
    dvs = VC // nz
    vmem = pl.BlockSpec(memory_space=pltpu.VMEM)
    hbm = pl.BlockSpec(memory_space=pl.ANY)
    dma = pltpu.SemaphoreType.DMA
    scratch = [
        pltpu.VMEM((tok, D), bf16),
        pltpu.VMEM((tok, D), bf16),
        pltpu.VMEM((D, 2 * DK), bf16),
        pltpu.VMEM((D, 2 * VC), bf16),
        pltpu.VMEM((share * VC, D), bf16),
        pltpu.VMEM((2, 3 * D), f32),
        pltpu.VMEM((nz, 2, MC), f32),
        pltpu.VMEM((tok, 2 * VC), bf16),
        pltpu.VMEM((tok, decay_in_weight.shape[1]), bf16),
        pltpu.VMEM((tok, 2 * DK), bf16),
        pltpu.VMEM((tok, 2 * DK), f32),
        pltpu.VMEM((2, tok, 2 * DK), bf16),
        pltpu.VMEM((tok, VC), f32),
        pltpu.VMEM((2, nb, VC, DK), f32),
        pltpu.VMEM((2, nb, 1, DK), f32),
        pltpu.VMEM((2, nb, VC, DK), f32),
        pltpu.VMEM((2, nb, 1, DK), f32),
        pltpu.VMEM((nz, 2 * dvs, DK), bf16),
        pltpu.VMEM((nz, 2 * dvs, DK), bf16),
        pltpu.VMEM((nz, 2 * dvs, DK), bf16),
        pltpu.VMEM((nz, 2 * dvs, DK), bf16),
        pltpu.VMEM((2, 2, DK), f32),
        pltpu.VMEM((2, nz, 2, DK), f32),
        pltpu.VMEM((nz, 2 * dvs, DK), bf16),
        pltpu.VMEM((nz, 2 * dvs, DK), bf16),
        pltpu.VMEM((share, 8, tok), f32),
        pltpu.VMEM((nt, TB, VC), f32),
        pltpu.VMEM((heads, TB, share * VC), f32),
        pltpu.VMEM((TB, D), f32),
        pltpu.VMEM((heads, 4, TB, D // 4), bf16),
        pltpu.VMEM((heads, 4, TB, D // 4), bf16),
        pltpu.VMEM((nt, TB, 8), f32),
        *[
            pltpu.VMEM(shape, kind)
            for shape, kind in (
                ((1, condition.shape[0]), f32),
                ((1, context_condition.shape[0]), f32),
                (mod_weight.shape, bf16),
                ((1, mod_bias.shape[0]), f32),
                (decay_weight.shape, bf16),
                (decay_bias.shape, f32),
                (extra_decay.shape, f32),
                ((1, norm_gain.shape[0]), f32),
                ((1, D), f32),
                ((1, D), f32),
            )
        ],
        pltpu.VMEM(context.shape, bf16),
        pltpu.VMEM((decay_in_weight.shape[1], D), bf16),
        pltpu.VMEM(row_tab.shape, f32),
        pltpu.VMEM(col_tab.shape, f32),
        pltpu.VMEM((2, tok, DK), f32),
        pltpu.VMEM((2, tok, DK), f32),
        pltpu.VMEM((2, tok, DK), f32),
        dma((20,)),
        dma((15,)),
        dma((15,)),
        dma((4 * nz,)),
        dma((2 * nt,)),
    ]
    in_specs = [hbm] * 20
    return pl.pallas_call(
        functools.partial(kernel, nz, nt, heads),
        out_shape=pltpu.VMEM((TB, D), bf16),
        in_specs=in_specs,
        out_specs=vmem,
        scratch_shapes=scratch,
        compiler_params=pltpu.CompilerParams(
            collective_id=0, has_side_effects=True, vmem_limit_bytes=58 * 1024 * 1024
        ),
        name="layer",
    )(
        latent,
        context,
        condition.reshape(1, -1),
        context_condition.reshape(1, -1),
        mod_weight,
        mod_bias.reshape(1, -1),
        query_weight,
        key_weight,
        value_weight,
        out_gate_weight,
        decay_in_weight.T,
        decay_weight,
        decay_bias,
        extra_decay,
        norm_gain.reshape(1, -1),
        out_weight,
        final_gain.reshape(1, -1),
        final_bias.reshape(1, -1),
        jnp.asarray(row_tab),
        jnp.asarray(col_tab),
    )


def solution(mesh):
    placed = (
        P(("grp", "sp", "tp"), None),
        P(("grp", "sp"), None),
        P(("grp", "sp")),
        P("sp"),
        P("sp", "tp"),
        P(),
        P("sp", None),
        P("sp", None),
        P(None, "tp"),
        P(None, "tp"),
        P(),
        P(),
        P(),
        P(None, None, "sp"),
        P(),
        P("tp", None),
        P(),
        P(),
    )
    return jax.shard_map(
        functools.partial(body, mesh.shape["sp"], mesh.shape["tp"]),
        mesh=mesh,
        in_specs=placed,
        out_specs=P(("grp", "sp", "tp"), None),
        check_vma=False,
    )
```

```python
import functools

import numpy as np
import jax
import jax.numpy as jnp
from jax import lax
from jax.experimental import pallas as pl
from jax.experimental.pallas import tpu as pltpu
from jax.sharding import PartitionSpec as P

ATTENTION_HEADS = 4
DV = 512
BLOCK = 64
GRID_W = 64

norm_eps = 1e-05
gate_scale = 16.0
rope_base = 10000.0
residual_scale = 2.0**0.5
highest = lax.Precision.HIGHEST
f32 = jnp.float32
bf16 = jnp.bfloat16

NT = (((1,), (1,)), ((), ()))
TN = (((0,), (0,)), ((), ()))


def dot(a, b, dims=None, precision=None):
    if dims is None:
        dims = (((1,), (0,)), ((), ()))
    return lax.dot_general(a, b, dims, precision=precision, preferred_element_type=f32)


def halves(a):
    high = a.astype(bf16)
    return high, (a - high.astype(f32)).astype(bf16)


def dot2(a, b, dims=None):
    high, low = halves(b)
    return dot(a, high, dims) + dot(a, low, dims)


def dot3(a, b, dims=None):
    a_high, a_low = halves(a)
    b_high, b_low = halves(b)
    return dot(a_high, b_high, dims) + (dot(a_high, b_low, dims) + dot(a_low, b_high, dims))


def log_sigmoid(v):
    return jnp.minimum(v, 0.0) - jnp.log1p(jnp.exp(-jnp.abs(v)))


def silu(v):
    return v / (1.0 + jnp.exp(-v))


def rotary_tables(rows, half):
    quarter = half // 2
    frequency = (rope_base ** (-np.arange(quarter, dtype=np.float64) / quarter)).astype(np.float32)

    def table(places):
        angle = (np.arange(places, dtype=np.float32)[:, None] * frequency).astype(np.float64)
        cosine = np.cos(angle)
        sine = np.sin(angle)
        return np.stack(
            [np.concatenate([cosine, cosine], 1), np.concatenate([-sine, sine], 1)]
        ).astype(np.float32)

    return table(rows), table(GRID_W)


def spread(n, j):
    long, short = n // 2, (n - 1) // 2
    right, left = (long, short) if j % 2 == 0 else (short, long)
    steps = {a: [a + 1] for a in range(1, right)} | {-a: [-a - 1] for a in range(1, left)}
    steps[0] = ([1] if right else []) + ([-1] if left else [])
    due = [o for a in range(1, long + 1) for o in (a, -a) if o <= right and o >= -left]
    return due, steps


def kernel(
    nz,
    nt,
    heads,
    lat_in,
    ctx_hbm,
    cond_hbm,
    ctx_cond_hbm,
    mod_w_hbm,
    mod_b_hbm,
    qw,
    kw,
    vw,
    gw,
    low_hbm,
    decay_w_hbm,
    decay_b_hbm,
    extra_hbm,
    gain_hbm,
    out_w,
    final_g_hbm,
    final_b_hbm,
    row_hbm,
    col_hbm,
    out,
    L,
    XM,
    W,
    VG,
    WO,
    M,
    mod_part,
    PVG,
    PLOW,
    PQK,
    QK,
    QD,
    O,
    U,
    TD,
    PF,
    OFF,
    LM,
    LR,
    CM,
    CR,
    DM,
    DR,
    RO,
    RR,
    SS,
    GT,
    GR,
    ACC,
    PS,
    PR,
    IV,
    cond,
    ctx_cond,
    mod_w,
    mod_b,
    decay_w,
    decay_b,
    extra,
    gain,
    final_g,
    final_b,
    CX,
    LOWT,
    RT,
    CT,
    EC,
    EI,
    EO,
    loc_sem,
    once_s,
    once_r,
    wz_r,
    lx_r,
):
    z = lax.axis_index("sp")
    t = lax.axis_index("tp")
    share = nt // heads
    h = t // share
    p = t % share
    core = t % 2
    x = t // 2
    nx = nt // 2
    partner = t + 1 - 2 * core
    D = lat_in.shape[1]
    TB = lat_in.shape[0]
    tok = TB * nt
    KR = qw.shape[0]
    DK = qw.shape[1] // heads
    HC = DK // 2
    VC = vw.shape[1]
    MC = mod_w_hbm.shape[1]
    nb = tok // BLOCK
    dvs = VC // nz
    pending = []
    MP, MG, WZ, WD, LX, LD, WOUT, LMS, CMS, DMS, ROS, SSS, GRS, PRS, DXS = range(15)

    def push(src, dst, ssem, rsem, **where):
        pltpu.make_async_remote_copy(
            src_ref=src,
            dst_ref=dst,
            send_sem=ssem,
            recv_sem=rsem,
            device_id=where,
            device_id_type=pl.DeviceIdType.MESH,
        ).start()

    def waiter(view, ssem, rsem):
        return pltpu.make_async_remote_copy(
            src_ref=view,
            dst_ref=view,
            send_sem=ssem,
            recv_sem=rsem,
            device_id={"tp": partner},
            device_id_type=pl.DeviceIdType.MESH,
        )

    def all_in(kind, view):
        waiter(view, once_s.at[kind], once_r.at[kind]).wait_recv()

    def sent(kind, view):
        pending.append(waiter(view, once_s.at[kind], once_r.at[kind]))

    def far_first(n):
        return sorted(range(1, n), key=lambda i: (-min(i, n - i), i))

    def at_z(i):
        return lax.rem(z + i + nz, nz)

    def at_t(i):
        return lax.rem(t + i + nt, nt)

    def at_x(i):
        return lax.rem(x + i + nx, nx)

    def al(v, m):
        return pl.multiple_of(v, m)

    def w_at(zz, j, parts=2):
        rows = KR // parts
        first = zz * KR + (j % parts) * rows
        return W.at[pl.ds(al(first, rows), rows), pl.ds((j // parts) * DK, DK)]

    def l_at(xx, j):
        rows = pl.ds(al((xx * 2 + j // 2) * TB, TB), TB)
        return L.at[rows, pl.ds((j % 2) * (D // 2), D // 2)]

    head_cols = pl.ds(al(h * DK, DK), DK)
    loads = [
        (cond_hbm, cond),
        (ctx_cond_hbm, ctx_cond),
        (mod_w_hbm, mod_w),
        (lat_in, L.at[pl.ds(al(t * TB, TB), TB), :]),
        (qw.at[:, head_cols], w_at(z, 0, 1)),
        (kw.at[:, head_cols], w_at(z, 1, 1)),
        (out_w, WO.at[pl.ds(al(p * VC, VC), VC), :]),
        (vw, VG.at[:, pl.ds(0, VC)]),
        (gw, VG.at[:, pl.ds(VC, VC)]),
        (ctx_hbm, CX),
        (low_hbm, LOWT),
        (mod_b_hbm, mod_b),
        (decay_w_hbm, decay_w),
        (decay_b_hbm, decay_b),
        (extra_hbm, extra),
        (gain_hbm, gain),
        (final_g_hbm, final_g),
        (final_b_hbm, final_b),
        (row_hbm, RT),
        (col_hbm, CT),
    ]
    local = [
        pltpu.make_async_copy(src, dst, loc_sem.at[i]) for i, (src, dst) in enumerate(loads)
    ]
    barrier = pltpu.get_barrier_semaphore()
    for i in far_first(nz):
        pl.semaphore_signal(
            barrier, inc=1, device_id={"sp": at_z(i)}, device_id_type=pl.DeviceIdType.MESH
        )
    for i in far_first(nt):
        pl.semaphore_signal(
            barrier, inc=1, device_id={"tp": at_t(i)}, device_id_type=pl.DeviceIdType.MESH
        )
    for copy in local[:6]:
        copy.start()
    for copy in local[:3]:
        copy.wait()

    both = jnp.concatenate([cond[...], ctx_cond[...], jnp.zeros((6, cond.shape[1]), f32)], axis=0)
    part = dot(silu(both).astype(bf16), mod_w[...])
    mod_part[z] = part[0:2]

    for copy in local[3:6]:
        copy.wait()
    pl.semaphore_wait(barrier, nz - 1 + nt - 1)

    for i in far_first(nz):
        push(mod_part.at[z], mod_part.at[z], once_s.at[MP], once_r.at[MP], sp=at_z(i))
    sent(MP, mod_part.at[pl.ds(0, nz - 1)])

    def ring(n, chunks, at, region, whole, far, sem_r, kind, share_kind):
        plans = [spread(n, j) for j in range(chunks)]

        def hand_on(o, j):
            src = region(at(-o), j)
            for c in plans[j][1].get(o, []):
                sem = sem_r.at[(c % n) * chunks + j]
                push(src, src, once_s.at[kind], sem, **far(c - o))

        def take(first, last):
            for i in range(first, min(last, n - 1)):
                for j in range(chunks):
                    o = plans[j][0][i]
                    sem = sem_r.at[(o % n) * chunks + j]
                    waiter(region(at(-o), j), once_s.at[kind], sem).wait_recv()
                    hand_on(o, j)
                src = whole(at(-plans[0][0][i]))
                push(src, src, once_s.at[share_kind], once_r.at[share_kind], tp=partner)

        return hand_on, take

    def l_whole(xx):
        return L.at[pl.ds(al(xx * 2 * TB, 2 * TB), 2 * TB), :]

    def w_whole(zz):
        return W.at[pl.ds(al(zz * KR, KR), KR), :]

    l_on, l_take = ring(
        nx, 4, at_x, l_at, l_whole, lambda i: {"tp": at_x(i) * 2 + core}, lx_r, LX, LD
    )
    w_on, w_take = ring(nz, 4, at_z, w_at, w_whole, lambda i: {"sp": at_z(i)}, wz_r, WZ, WD)
    own_rows = L.at[pl.ds(al(t * TB, TB), TB), :]
    rest = pl.ds(0, (2 * nx - 1) * TB)

    def load_rest():
        for copy in local[6:]:
            copy.start()

    @pl.when(core == 0)
    def _():
        for j in range(2):
            l_on(0, j)
        push(own_rows, own_rows, once_s.at[LD], once_r.at[LD], tp=partner)
        all_in(LD, L.at[pl.ds(0, TB), :])
        for j in range(2, 4):
            l_on(0, j)
        load_rest()
        l_take(0, 4)

    @pl.when(core == 1)
    def _():
        push(own_rows, own_rows, once_s.at[LD], once_r.at[LD], tp=partner)
        for j in range(4):
            w_on(0, j)
        load_rest()
        w_take(0, 6)

    def modulation_sums():
        all_in(MP, mod_part.at[pl.ds(0, nz - 1)])
        sums = mod_part[0]
        for i in range(1, nz):
            sums = sums + mod_part[i]
        cols = pl.ds(al(t * MC, 128), MC)
        M[:, cols] = sums
        for i in far_first(nt):
            push(M.at[:, cols], M.at[:, cols], once_s.at[MG], once_r.at[MG], tp=at_t(i))
        sent(MG, M.at[:, pl.ds(0, (nt - 1) * MC)])

    modulation_sums()

    @pl.when(core == 0)
    def _():
        l_take(4, nx - 1)

    @pl.when(core == 1)
    def _():
        w_take(6, 12)

    local[6].wait()
    proj_rows = WO.at[pl.ds(al(p * VC, VC), VC), :]
    for i in range(1, share):
        push(
            proj_rows,
            proj_rows,
            once_s.at[WOUT],
            once_r.at[WOUT],
            tp=h * share + lax.rem(p + i, share),
        )
    sent(WOUT, WO.at[pl.ds(0, (share - 1) * VC), :])
    all_in(MG, M.at[:, pl.ds(0, (nt - 1) * MC)])
    for copy in local[7:]:
        copy.wait()

    mod = M[...] + mod_b[...]
    shift, scale = mod[:, :D], 1.0 + mod[:, D : 2 * D]
    bias = decay_b[:, pl.ds(al(h * DK, DK), DK)]
    rank = decay_w.shape[1]
    zero = jnp.zeros((rank, DK), bf16)
    maps = [
        jnp.concatenate([decay_w[0, :, head_cols], zero], axis=0),
        jnp.concatenate([zero, decay_w[1, :, head_cols]], axis=0),
    ]

    def triangles(size):
        row = lax.broadcasted_iota(jnp.int32, (size, size), 0)
        col = lax.broadcasted_iota(jnp.int32, (size, size), 1)
        return row >= col, row <= col

    low_b, up_b = triangles(BLOCK)
    added = [extra[d, pl.ds(h, 1), :] for d in range(2)]

    def decays(low, d):
        return log_sigmoid(dot(low, maps[d]) + bias[d : d + 1]) * (1.0 / gate_scale)

    @pl.when(core == 1)
    def _():
        all_in(LD, L.at[rest, :])

    def message(forward, backward):
        return jnp.concatenate(
            [forward.reshape(nz, dvs, DK), backward.reshape(nz, dvs, DK)], axis=1
        ).astype(bf16)

    def context_states():
        ctx_rows = (CX[...].astype(f32) * scale[1:2] + shift[1:2]).astype(bf16)
        ctx_values = dot(ctx_rows, VG[:, 0:VC]).astype(bf16)
        ctx_low = dot(ctx_rows, LOWT[...], NT).astype(bf16)
        CB = ctx_hbm.shape[0]
        low_c, up_c = triangles(CB)
        cum_f = dot(low_c.astype(f32), decays(ctx_low, 0), precision=highest)
        cum_b = dot(up_c.astype(f32), decays(ctx_low, 1), precision=highest)
        tot_cf, tot_cb = cum_f[CB - 1 : CB], cum_b[0:1]
        DM[1, 0:1, :] = tot_cf
        DM[1, 1:2, :] = tot_cb
        ctx_keys = dot(ctx_rows, W[:, DK : 2 * DK]).astype(bf16).astype(f32)
        CM[...] = message(
            dot2(ctx_values, ctx_keys * jnp.exp(tot_cf - cum_f), TN),
            dot2(ctx_values, ctx_keys * jnp.exp(tot_cb - cum_b), TN),
        )
        for i in far_first(nz):
            push(CM.at[at_z(i)], CR.at[z], once_s.at[CMS], once_r.at[CMS], sp=at_z(i))
        CR[z] = CM[z]

    tiles = max(1, tok // 128)
    TR = tok // tiles

    def values_tile(i):
        rows = pl.ds(i * TR, TR)
        rounded = (L[rows, :].astype(f32) * scale[0:1] + shift[0:1]).astype(bf16)
        XM[rows, :] = rounded
        PVG[rows, :] = dot(rounded, VG[...]).astype(bf16)
        PLOW[rows, :] = dot(rounded, LOWT[...], NT).astype(bf16)

    def decays_tile(i):
        low = PLOW[pl.ds(i * TR, TR), :]
        for d, mask in ((0, low_b), (1, up_b)):
            steps = decays(low, d)
            for b in range(i * TR // BLOCK, (i + 1) * TR // BLOCK):
                at = b * BLOCK - i * TR
                ex = added[d][:, b * BLOCK : (b + 1) * BLOCK]
                cum = dot(mask.astype(f32), steps[at : at + BLOCK], precision=highest) + jnp.sum(
                    jnp.where(mask, ex, 0.0), axis=1, keepdims=True
                )
                total = cum[BLOCK - 1 : BLOCK] if d == 0 else cum[0:1]
                block_rows = slice(b * BLOCK, (b + 1) * BLOCK)
                EC[d, block_rows, :] = jnp.exp(cum)
                EI[d, block_rows, :] = jnp.exp(-cum)
                EO[d, block_rows, :] = jnp.exp(total - cum)
                TD[d, b] = total

    pieces = [f for i in range(tiles) for f in ((values_tile, i), (decays_tile, i))]
    for n, (piece, i) in enumerate(pieces):
        piece(i)
        if n < 3:
            first, last = 12 + n, (13 + n if n + 1 < min(3, len(pieces)) else nz - 1)

            @pl.when(core == 1)
            def _():
                w_take(first, last)
                if last == nz - 1:
                    context_states()

    @pl.when(core == 0)
    def _():
        all_in(WD, W.at[pl.ds(0, (nz - 1) * KR), :])
        context_states()

    sum_f, sum_b = jnp.zeros((1, DK), f32), jnp.zeros((1, DK), f32)
    for b in range(nb):
        OFF[0, b] = sum_f
        OFF[1, nb - 1 - b] = sum_b
        sum_f = sum_f + TD[0, b]
        sum_b = sum_b + TD[1, nb - 1 - b]
    DM[0, 0:1, :] = sum_f
    DM[0, 1:2, :] = sum_b
    for i in far_first(nz):
        push(DM.at[core], DR.at[core, z], once_s.at[DMS], once_r.at[DMS], sp=at_z(i))
    sent(CMS, CM.at[pl.ds(0, nz - 1)])
    sent(DMS, DR.at[0, pl.ds(0, nz - 1)])
    DR[core, z] = DM[core]

    QT = min(tok, 256)

    def project_qk(i, carry):
        rows = pl.ds(al(i * QT, QT), QT)
        PQK[rows, :] = dot(XM[rows, :], W[...]).astype(bf16)
        return carry

    lax.fori_loop(0, tok // QT, project_qk, 0)

    half = DK // 2
    for b in range(nb):
        rows = slice(b * BLOCK, (b + 1) * BLOCK)
        place = pl.ds(z * nb + b, 1)
        row_cos, row_sin = RT[0, place, :], RT[1, place, :]

        def rotated(values):
            first, second = values[:, :half], values[:, half:]
            return jnp.concatenate(
                [
                    first * row_cos + pltpu.roll(first, half // 2, 1) * row_sin,
                    second * CT[0] + pltpu.roll(second, half // 2, 1) * CT[1],
                ],
                axis=1,
            )

        q = rotated(PQK[rows, :DK].astype(f32)) * DK ** (-0.5)
        k = rotated(PQK[rows, DK:].astype(f32))
        v = PVG[rows, 0:VC]
        QK[rows, :DK] = q
        QK[rows, DK:] = k
        for d in range(2):
            U[d, b] = dot2(v, k * EO[d, rows, :], TN)

    fwd, bwd = jnp.zeros((VC, DK), f32), jnp.zeros((VC, DK), f32)
    for b in range(nb):
        e = nb - 1 - b
        PF[0, b] = fwd
        PF[1, e] = bwd
        fwd = jnp.exp(TD[0, b]) * fwd + U[0, b]
        bwd = jnp.exp(TD[1, e]) * bwd + U[1, e]
    LM[...] = message(fwd, bwd)
    for i in far_first(nz):
        push(LM.at[at_z(i)], LR.at[z], once_s.at[LMS], once_r.at[LMS], sp=at_z(i))
    sent(LMS, LM.at[pl.ds(0, nz - 1)])
    LR[z] = LM[z]

    for b in range(nb):
        rows = slice(b * BLOCK, (b + 1) * BLOCK)
        q, k = QK[rows, :DK], QK[rows, DK:]
        scores = jnp.zeros((BLOCK, BLOCK), f32)
        total = jnp.zeros((BLOCK, VC), f32)
        for d, mask in ((0, low_b), (1, up_b)):
            q_in = q * EC[d, rows, :]
            scores = scores + jnp.where(mask, dot3(q_in, k * EI[d, rows, :], NT), 0.0)
            total = total + dot3(q_in, PF[d, b], NT)
            high, low = halves(q_in * jnp.exp(OFF[d, b]))
            QD[0, rows, d * DK : (d + 1) * DK] = high
            QD[1, rows, d * DK : (d + 1) * DK] = low
        high, low = halves(scores)
        v = PVG[rows, 0:VC]
        O[rows, :] = total + (dot(high, v) + dot(low, v))

    all_in(CMS, CR.at[pl.ds(0, nz - 1)])
    all_in(DMS, DR.at[0, pl.ds(0, nz - 1)])
    push(DR.at[core], DR.at[core], once_s.at[DXS], once_r.at[DXS], tp=partner)
    sent(DXS, DR.at[0])
    all_in(LMS, LR.at[pl.ds(0, nz - 1)])
    all_in(DXS, DR.at[0])

    def context_chain(s, carry):
        fwd, bwd = carry
        e = nz - 1 - s
        fwd = jnp.exp(DR[1, s, 0:1]) * fwd + CR[s].astype(f32)[:dvs]
        bwd = jnp.exp(DR[1, e, 1:2]) * bwd + CR[e].astype(f32)[dvs:]
        return fwd, bwd

    slice0 = jnp.zeros((dvs, DK), f32)
    fwd, bwd = lax.fori_loop(0, nz, context_chain, (slice0, slice0))
    fwd_in, bwd_in = [], [None] * nz
    for s in range(nz):
        e = nz - 1 - s
        fwd_in.append(fwd)
        bwd_in[e] = bwd
        fwd = jnp.exp(DR[0, s, 0:1]) * fwd + LR[s].astype(f32)[:dvs]
        bwd = jnp.exp(DR[0, e, 1:2]) * bwd + LR[e].astype(f32)[dvs:]
    for s in range(nz):
        RO[s] = jnp.concatenate([fwd_in[s], bwd_in[s]], axis=0).astype(bf16)
    for i in far_first(nz):
        push(RO.at[at_z(i)], RR.at[z], once_s.at[ROS], once_r.at[ROS], sp=at_z(i))
    sent(ROS, RO.at[pl.ds(0, nz - 1)])
    RR[z] = RO[z]
    gate_rows = silu(PVG[:, VC:].astype(f32)) * gain[:, pl.ds(al(p * VC, VC), VC)]
    all_in(ROS, RR.at[pl.ds(0, nz - 1)])
    back = RR[...].astype(f32)
    start = jnp.concatenate(
        [back[:, :dvs].reshape(VC, DK), back[:, dvs:].reshape(VC, DK)], axis=1
    ).astype(bf16)
    mixture = O[...] + (dot(QD[0], start, NT) + dot(QD[1], start, NT))

    SS[p] = dot(jnp.ones((8, VC), f32), mixture * mixture, NT, precision=highest)[0:1]
    for i in range(1, share):
        push(
            SS.at[p],
            SS.at[p],
            once_s.at[SSS],
            once_r.at[SSS],
            tp=h * share + lax.rem(p + i, share),
        )
    sent(SSS, SS.at[pl.ds(0, share - 1)])
    GT[...] = (mixture * gate_rows).reshape(nt, TB, VC)

    def owner(q, j):
        chip = jnp.where(q // 2 == 0, 2 * h - j + nx, 2 * h + 1 + j)
        return lax.rem(chip, nx) * 2 + q % 2

    lanes = pl.ds(al(p * VC, VC), VC)
    for i in range(1, share):
        q = lax.rem(p + i, share)
        for j in range(heads):
            push(
                GT.at[owner(q, j)],
                GR.at[j, :, lanes],
                once_s.at[GRS],
                once_r.at[GRS],
                tp=h * share + q,
            )
    sent(GRS, GT.at[pl.ds(0, (share - 1) * heads)])
    for j in range(heads):
        GR[j, :, lanes] = GT[owner(p, j)]
    all_in(SSS, SS.at[pl.ds(0, share - 1)])
    squares = SS[0]
    for i in range(1, share):
        squares = squares + SS[i]
    inverse = lax.rsqrt(squares / (share * VC) + norm_eps)
    IV[...] = jnp.broadcast_to(inverse, (8, tok)).T.reshape(nt, TB, 8)
    all_in(WOUT, WO.at[pl.ds(0, (share - 1) * VC), :])
    all_in(GRS, GT.at[pl.ds(0, (share - 1) * heads)])

    left = jnp.concatenate(
        [(GR[j] * IV[owner(p, j)][:, 0:1]).astype(bf16) for j in range(heads)], axis=0
    )
    NC = D // 4
    for n in range(4):
        partial = dot(left, WO[:, n * NC : (n + 1) * NC]).reshape(heads, TB, NC)
        ACC[:, n * NC : (n + 1) * NC] = partial[0]
        PS[:, n] = partial.astype(bf16)
        for j in range(heads - 1, 0, -1):
            push(PS.at[j, n], PR.at[j, n], once_s.at[PRS], once_r.at[PRS], tp=owner(p, j))
    branch = ACC[...]
    if heads > 1:
        sent(PRS, PS.at[pl.ds(0, heads - 1)])
        all_in(PRS, PR.at[pl.ds(0, heads - 1)])
    for j in range(1, heads):
        branch = branch + jnp.concatenate([PR[j, n].astype(f32) for n in range(4)], axis=1)
    own = L[pl.ds(al(t * TB, TB), TB), :].astype(f32)
    gates = M[0:1, 2 * D :] + mod_b[:, 2 * D :]
    summed = residual_scale * own + gates * branch
    centered = summed - jnp.mean(summed, axis=1, keepdims=True)
    variance = jnp.mean(centered * centered, axis=1, keepdims=True)
    out[...] = (
        centered * lax.rsqrt(variance + norm_eps) * final_g[...] + final_b[...]
    ).astype(out.dtype)
    for copy in pending:
        copy.wait_send()

    @pl.when(core == 0)
    def _():
        waiter(L.at[pl.ds(0, 2 * (nx - 1) * TB), :], once_s.at[LX], once_r.at[LX]).wait_send()
        waiter(L.at[rest, :], once_s.at[LD], once_r.at[LD]).wait_send()

    @pl.when(core == 1)
    def _():
        view = W.at[pl.ds(0, (nz - 1) * KR), :]
        waiter(view, once_s.at[WZ], once_r.at[WZ]).wait_send()
        waiter(view, once_s.at[WD], once_r.at[WD]).wait_send()
        waiter(L.at[pl.ds(0, TB), :], once_s.at[LD], once_r.at[LD]).wait_send()


def body(
    nz,
    nt,
    latent,
    context,
    condition,
    context_condition,
    mod_weight,
    mod_bias,
    query_weight,
    key_weight,
    value_weight,
    out_gate_weight,
    decay_in_weight,
    decay_weight,
    decay_bias,
    extra_decay,
    norm_gain,
    out_weight,
    final_gain,
    final_bias,
):
    heads = ATTENTION_HEADS
    share = nt // heads
    D = latent.shape[1]
    TB = latent.shape[0]
    tok = TB * nt
    DK = query_weight.shape[1] // heads
    VC = value_weight.shape[1]
    MC = mod_weight.shape[1]
    nb = tok // BLOCK
    row_tab, col_tab = rotary_tables(nz * nb, DK // 2)
    dvs = VC // nz
    vmem = pl.BlockSpec(memory_space=pltpu.VMEM)
    hbm = pl.BlockSpec(memory_space=pl.ANY)
    dma = pltpu.SemaphoreType.DMA
    scratch = [
        pltpu.VMEM((tok, D), bf16),
        pltpu.VMEM((tok, D), bf16),
        pltpu.VMEM((D, 2 * DK), bf16),
        pltpu.VMEM((D, 2 * VC), bf16),
        pltpu.VMEM((share * VC, D), bf16),
        pltpu.VMEM((2, 3 * D), f32),
        pltpu.VMEM((nz, 2, MC), f32),
        pltpu.VMEM((tok, 2 * VC), bf16),
        pltpu.VMEM((tok, decay_in_weight.shape[1]), bf16),
        pltpu.VMEM((tok, 2 * DK), bf16),
        pltpu.VMEM((tok, 2 * DK), f32),
        pltpu.VMEM((2, tok, 2 * DK), bf16),
        pltpu.VMEM((tok, VC), f32),
        pltpu.VMEM((2, nb, VC, DK), f32),
        pltpu.VMEM((2, nb, 1, DK), f32),
        pltpu.VMEM((2, nb, VC, DK), f32),
        pltpu.VMEM((2, nb, 1, DK), f32),
        pltpu.VMEM((nz, 2 * dvs, DK), bf16),
        pltpu.VMEM((nz, 2 * dvs, DK), bf16),
        pltpu.VMEM((nz, 2 * dvs, DK), bf16),
        pltpu.VMEM((nz, 2 * dvs, DK), bf16),
        pltpu.VMEM((2, 2, DK), f32),
        pltpu.VMEM((2, nz, 2, DK), f32),
        pltpu.VMEM((nz, 2 * dvs, DK), bf16),
        pltpu.VMEM((nz, 2 * dvs, DK), bf16),
        pltpu.VMEM((share, 1, tok), f32),
        pltpu.VMEM((nt, TB, VC), f32),
        pltpu.VMEM((heads, TB, share * VC), f32),
        pltpu.VMEM((TB, D), f32),
        pltpu.VMEM((heads, 4, TB, D // 4), bf16),
        pltpu.VMEM((heads, 4, TB, D // 4), bf16),
        pltpu.VMEM((nt, TB, 8), f32),
        *[
            pltpu.VMEM(shape, kind)
            for shape, kind in (
                ((1, condition.shape[0]), f32),
                ((1, context_condition.shape[0]), f32),
                (mod_weight.shape, bf16),
                ((1, mod_bias.shape[0]), f32),
                (decay_weight.shape, bf16),
                (decay_bias.shape, f32),
                (extra_decay.shape, f32),
                ((1, norm_gain.shape[0]), f32),
                ((1, D), f32),
                ((1, D), f32),
            )
        ],
        pltpu.VMEM(context.shape, bf16),
        pltpu.VMEM((decay_in_weight.shape[1], D), bf16),
        pltpu.VMEM(row_tab.shape, f32),
        pltpu.VMEM(col_tab.shape, f32),
        pltpu.VMEM((2, tok, DK), f32),
        pltpu.VMEM((2, tok, DK), f32),
        pltpu.VMEM((2, tok, DK), f32),
        dma((20,)),
        dma((15,)),
        dma((15,)),
        dma((4 * nz,)),
        dma((2 * nt,)),
    ]
    in_specs = [hbm] * 20
    return pl.pallas_call(
        functools.partial(kernel, nz, nt, heads),
        out_shape=pltpu.VMEM((TB, D), bf16),
        in_specs=in_specs,
        out_specs=vmem,
        scratch_shapes=scratch,
        compiler_params=pltpu.CompilerParams(
            collective_id=0, has_side_effects=True, vmem_limit_bytes=58 * 1024 * 1024
        ),
        name="layer",
    )(
        latent,
        context,
        condition.reshape(1, -1),
        context_condition.reshape(1, -1),
        mod_weight,
        mod_bias.reshape(1, -1),
        query_weight,
        key_weight,
        value_weight,
        out_gate_weight,
        decay_in_weight.T,
        decay_weight,
        decay_bias,
        extra_decay,
        norm_gain.reshape(1, -1),
        out_weight,
        final_gain.reshape(1, -1),
        final_bias.reshape(1, -1),
        jnp.asarray(row_tab),
        jnp.asarray(col_tab),
    )


def solution(mesh):
    placed = (
        P(("grp", "sp", "tp"), None),
        P(("grp", "sp"), None),
        P(("grp", "sp")),
        P("sp"),
        P("sp", "tp"),
        P(),
        P("sp", None),
        P("sp", None),
        P(None, "tp"),
        P(None, "tp"),
        P(),
        P(),
        P(),
        P(None, None, "sp"),
        P(),
        P("tp", None),
        P(),
        P(),
    )
    return jax.shard_map(
        functools.partial(body, mesh.shape["sp"], mesh.shape["tp"]),
        mesh=mesh,
        in_specs=placed,
        out_specs=P(("grp", "sp", "tp"), None),
        check_vma=False,
    )
```
